32 devices in a mesh: ep: 4 (over y, x), tp: 8 (over z, core).
Axes of the slice: x: 2, y: 2, z: 4, core: 2. Of those that a mesh axis runs over, the one named last changes fastest.
Arguments:
- tokens: bfloat16 [64, 4096], P('ep'), may hold values from -150 to 150
- query_weight: bfloat16 [4096, 1024], P('tp'), may hold values from -0.09375 to 0.09375
- key_weight: bfloat16 [4096, 1024], P('tp'), may hold values from -0.09375 to 0.09375
- value_weight: bfloat16 [4096, 2048], P(None, 'tp'), may hold values from -0.09375 to 0.09375
- decay_down: bfloat16 [4096, 16], replicated, may hold values from -0.09375 to 0.09375
- decay_up: float32 [16, 1024], replicated, may hold values from -3 to 3
- decay_bias: float32 [1024], replicated, may hold values from -8 to 4
- old_state: float32 [64, 256, 2048], P('ep', None, 'tp'), may hold values from -8 to 8
- out_weight: bfloat16 [2048, 4096], P('tp'), may hold values from -0.1875 to 0.1875
- norm_gain: float32 [4096], replicated, may hold values from 0.2 to 4
- router_weight: bfloat16 [4096, 4], replicated, may hold values from -0.09375 to 0.09375
- routing: int32 [64, 2], P('ep'), may hold values from 0 to 3, all different within a row; in each aligned block of 16 rows (0 to 15, 16 to 31, ...) at most 16 rows name the same one
- glu_weight: bfloat16 [4, 4096, 2048], P('ep', None, 'tp'), may hold values from -0.25 to 0.25
- linear_weight: bfloat16 [4, 4096, 2048], P('ep', None, 'tp'), may hold values from -0.25 to 0.25
- down_weight: bfloat16 [4, 2048, 4096], P('ep', 'tp'), may hold values from -0.01953125 to 0.01953125
- final_gain: float32 [4096], replicated, may hold values from 0.1 to 1.9
Outputs:
- layer_out: bfloat16 [64, 4096], P('ep', 'tp')
- new_state: float32 [64, 256, 2048], P('ep', None, 'tp')
The draws below stay inside these ranges and needn't reach their ends.
Inputs may be any that keep to these rules, and one draw needn't show every extreme that they name: `routing`: within the rows of one device (aligned blocks of 16 rows) no expert is named by more than 16 rows, and at least one block reaches that bound; each row names 2 different experts.
All inputs are finite; a program needn't handle non-finite values.
Results may differ from the reference program's by a relative error of at most 0.015.
Values may be sent and summed in bfloat16 or wider, within the bound.
A program may use at most 64 MiB of HBM per device.

```python
import math
import jax
import jax.numpy as jnp
import numpy as np
from jax import lax

D = 4096
HEADS = 4
HEAD_DK = 256
HEAD_DV = 512
DK = 1024
DV = 2048
RANK = 16
FF = 2048
TOP = 2
SEQ_DEV = 16
SEQS = 64
EXPERTS = 4
CAP = 16


def draw_tokens(key, part):
    row_key, column_key, base_key = jax.random.split(jax.random.fold_in(key, 11), 3)
    position = jnp.arange(D, dtype=jnp.float32) / D
    column = 0.25 * jnp.exp(position * jnp.log(10.0)) * jax.random.uniform(column_key, (D,), jnp.float32, 0.7, 1.3)
    row_scale = jnp.exp(jax.random.uniform(row_key, (SEQS, 1), jnp.float32, -1.15, 1.15))
    base = jnp.clip(jax.random.normal(base_key, (SEQS, D), jnp.float32), -6.0, 6.0)
    return (base * row_scale * column[None, :]).astype(jnp.bfloat16)


def draw_norm_gain(key, part):
    position = jnp.arange(D, dtype=jnp.float32) / D
    rough_key = jax.random.fold_in(key, 23)
    trend = 0.5 * jnp.exp(position * jnp.log(4.0))
    rough = jax.random.uniform(rough_key, (D,), jnp.float32, 0.8, 1.2)
    return (trend * rough).astype(jnp.float32)


def strengthened(values, key, source, target, blocks, factor):
    def block_of(dim):
        return (jnp.arange(values.shape[dim]) // (values.shape[dim] // blocks)).reshape((-1,) + (1,) * (values.ndim - 1 - dim))

    first = jax.random.permutation(key, blocks)[block_of(target)]
    second = (block_of(target) + blocks // 2) % blocks
    return jnp.where((block_of(source) == first) | (block_of(source) == second), factor * values, values)


def shard_levels(key, dims, cuts, least, largest):
    factor_of, own = 1.0, jax.random.fold_in(key, 6)
    for dim, parts in cuts:
        steps = jnp.exp(jax.random.uniform(jax.random.fold_in(own, dim), (parts,), jnp.float32, least / len(cuts), largest / len(cuts)))
        factor_of = factor_of * jnp.repeat(steps, dims[dim] // parts).reshape([-1 if axis == dim else 1 for axis in range(len(dims))])
    return factor_of


def shared_out(rng, own, number, rows, number_of, top, bound, slope):
    ranking = jax.random.permutation(rng, number_of)
    packed, usual = load_shares(number_of, rows * top, bound, slope, True), load_shares(number_of, rows * top, bound, slope, False)
    places = jnp.arange(number_of)

    def named(sizes, rotation):
        used = int((sizes > 0).sum())
        fixed = max(1, used // 4)
        moved = fixed + (places - fixed + rotation * (used - fixed)) % max(1, number_of - fixed)
        return jnp.zeros((number_of,), jnp.int32).at[ranking[jnp.where(places < fixed, places, moved)]].set(jnp.asarray(sizes, jnp.int32))

    sizes = jnp.where(number % 4 == 0, named(packed, number // 4), named(usual, number - number // 4 - 1))
    mixed = jax.random.permutation(jax.random.fold_in(own, 3), number_of)
    source_of, taker = mixed[0:number_of // 2 * 2:2], mixed[1:number_of // 2 * 2:2]
    room = jnp.minimum(sizes[source_of] - 1, bound - sizes[taker]) // 2
    room = jnp.where((source_of == ranking[0]) | (taker == ranking[0]) | (sizes[taker] == 0), 0, jnp.maximum(room, 0))
    moved = jax.random.randint(jax.random.fold_in(own, 4), (number_of // 2,), 0, 1 << 20) % (room + 1)
    sizes = sizes.at[source_of].add(-moved).at[taker].add(moved)
    items = jnp.searchsorted(jnp.cumsum(sizes), jnp.arange(rows * top), side="right").astype(jnp.int32)
    table = items.reshape(top, rows).T
    table = table[jax.random.permutation(jax.random.fold_in(own, 1), rows)]
    rotation = jax.random.randint(jax.random.fold_in(own, 2), (rows, 1), 0, top)
    return jnp.take_along_axis(table, (jnp.arange(top)[None, :] + rotation) % top, axis=1)


def load_shares(number_of, total, limit, lean, full):
    portions = [(1 << 20) // math.isqrt(grade ** lean) + 1 for grade in range(1, number_of + 1)]
    largest = limit if full else min(limit, max(-(-total // number_of), total * portions[0] // sum(portions)))
    least = 1 if total - largest >= number_of - 1 else 0
    given, surplus = [largest] + [least] * (number_of - 1), total - largest - least * (number_of - 1)
    while surplus > 0:
        candidates = [i for i in range(1, number_of) if given[i] < largest] or [i for i in range(1, number_of) if given[i] < limit]
        pool, remaining = sum([portions[i] for i in candidates]), surplus
        for i in candidates:
            extra = min(limit - given[i], max(1, remaining * portions[i] // pool), surplus)
            given[i] = given[i] + extra
            surplus = surplus - extra
    return np.array(given)


def gaussian(key, dims, scale, bound, pieces=(), kind=jnp.bfloat16):
    level = shard_levels(key, dims, pieces, -0.22, 0.18) if pieces else 1.0
    array = jax.random.normal(key, dims, jnp.float32) * scale * level
    return jnp.minimum(jnp.maximum(array, -bound), bound).astype(kind)


def heavy_noise(key, dims, width, bound, cuts, heavy, held_as=jnp.bfloat16):
    array = width * jax.random.normal(key, dims, jnp.float32)
    if cuts:
        array = array * shard_levels(key, dims, cuts, -0.22, 0.18)
    return jnp.clip(strengthened(array, jax.random.fold_in(key, 3), *heavy), -bound, bound).astype(held_as)


def setup_inputs(seed: int = 0) -> dict:
    seeds = jax.random.split(jax.random.key(seed), 17)
    tokens = draw_tokens(jax.random.fold_in(seeds[16], 71), 0)
    query_weight = gaussian(seeds[1], (D, DK), D ** -0.5, 0.09375, ((0, 8),))
    key_weight = gaussian(seeds[2], (D, DK), D ** -0.5, 0.09375, ((0, 8),))
    value_weight = gaussian(seeds[3], (D, DV), D ** -0.5, 0.09375, ((1, 8),))
    decay_down = gaussian(seeds[4], (D, RANK), D ** -0.5, 0.09375)
    decay_up = gaussian(seeds[5], (RANK, DK), (RANK // 4) ** -0.5, 3.0, (), jnp.float32)
    decay_bias = jnp.clip(jax.random.uniform(seeds[6], (DK,), jnp.float32, -8.0, 4.0), -8.0, 4.0)
    old_state = gaussian(seeds[7], (SEQS, HEAD_DK, DV), 2.0, 8.0, ((0, 4), (2, 8)), jnp.float32)
    out_weight = heavy_noise(seeds[8], (DV, D), DV ** -0.5, 0.1875, ((0, 8),), (0, 1, 8, 2.0))
    norm_gain = draw_norm_gain(jax.random.fold_in(seeds[16], 71), 0)
    router_weight = gaussian(seeds[10], (D, EXPERTS), D ** -0.5, 0.09375)
    routing_keys = jax.random.split(jax.random.fold_in(seeds[11], 1), SEQS // SEQ_DEV)
    routing_turns = jax.random.permutation(jax.random.fold_in(seeds[11], 3), SEQS // SEQ_DEV)
    routing = jax.vmap(lambda own, number: shared_out(jax.random.fold_in(seeds[11], 2), own, number, SEQ_DEV, EXPERTS, TOP, CAP, 2))(routing_keys, routing_turns).reshape((SEQS, TOP))
    glu_weight = gaussian(seeds[12], (EXPERTS, D, FF), (D // 9) ** -0.5, 0.25, ((0, 4), (2, 8)))
    linear_weight = gaussian(seeds[13], (EXPERTS, D, FF), (D // 9) ** -0.5, 0.25, ((0, 4), (2, 8)))
    down_weight = heavy_noise(seeds[14], (EXPERTS, FF, D), (FF * 100) ** -0.5, 0.01953125, ((0, 4), (1, 8)), (1, 2, 8, 2.0))
    final_gain = jnp.clip(1.0 + 0.18 * jax.random.normal(seeds[15], (D,), jnp.float32), 0.1, 1.9)
    return {"tokens": tokens, "query_weight": query_weight, "key_weight": key_weight, "value_weight": value_weight, "decay_down": decay_down, "decay_up": decay_up, "decay_bias": decay_bias, "old_state": old_state, "out_weight": out_weight, "norm_gain": norm_gain, "router_weight": router_weight, "routing": routing, "glu_weight": glu_weight, "linear_weight": linear_weight, "down_weight": down_weight, "final_gain": final_gain}


ALPHA = 2.0 ** 0.25
TAU = 16.0
LIMIT = 7.0
SLOPE = 1.702
EPSILON = 1e-05

def layer_norm(inputs, gain):
    mean = lax.optimization_barrier(jnp.mean(inputs, axis=-1, keepdims=True))
    centered = inputs - mean
    variance = lax.optimization_barrier(jnp.mean(centered * centered, axis=-1, keepdims=True))
    return centered * lax.rsqrt(variance + EPSILON) * gain

def clamped_unit(glu_pre, linear_pre):
    glu = jnp.minimum(glu_pre, LIMIT)
    linear = jnp.clip(linear_pre, -LIMIT, LIMIT)
    return glu * jax.nn.sigmoid(SLOPE * glu) * (linear + 1.0)

def reference(tokens, query_weight, key_weight, value_weight, decay_down, decay_up, decay_bias, old_state, out_weight, norm_gain, router_weight, routing, glu_weight, linear_weight, down_weight, final_gain):
    query = jnp.dot(tokens, query_weight, preferred_element_type=jnp.float32).astype(jnp.bfloat16)
    keys = jnp.dot(tokens, key_weight, preferred_element_type=jnp.float32).astype(jnp.bfloat16)
    values = jnp.dot(tokens, value_weight, preferred_element_type=jnp.float32).astype(jnp.bfloat16)
    low_rank = jnp.dot(tokens, decay_down, preferred_element_type=jnp.float32)
    decay = jnp.exp(jax.nn.log_sigmoid(jnp.dot(low_rank, decay_up, precision=lax.Precision.HIGHEST) + decay_bias) / TAU)
    state_parts = []
    mixed_parts = []
    for head in range(HEADS):
        key_cols = slice(head * HEAD_DK, (head + 1) * HEAD_DK)
        value_cols = slice(head * HEAD_DV, (head + 1) * HEAD_DV)
        updated = decay[:, key_cols, None] * old_state[:, :, value_cols] + keys[:, key_cols].astype(jnp.float32)[:, :, None] * values[:, value_cols].astype(jnp.float32)[:, None, :]
        state_parts.append(updated)
        mixed_parts.append(jnp.einsum('bi,bic->bc', query[:, key_cols].astype(jnp.float32), updated, precision=lax.Precision.HIGHEST) * HEAD_DK ** (-0.5))
    new_state = jnp.concatenate(state_parts, axis=2)
    mixed = jnp.concatenate(mixed_parts, axis=1).astype(jnp.bfloat16)
    hidden_in = ALPHA * tokens.astype(jnp.float32) + jnp.dot(mixed, out_weight, preferred_element_type=jnp.float32)
    normed = layer_norm(hidden_in, norm_gain).astype(jnp.bfloat16)
    logits = jnp.dot(normed, router_weight, preferred_element_type=jnp.float32)
    picked = jnp.take_along_axis(logits, routing, axis=1)
    raised = jnp.exp(picked)
    gates = raised / lax.optimization_barrier(jnp.sum(raised, axis=1, keepdims=True))
    expert_ids = jnp.arange(EXPERTS, dtype=jnp.int32)
    chosen = (routing[:, :, None] == expert_ids[None, None, :]).astype(jnp.float32)
    share = lax.optimization_barrier(jnp.sum(chosen * gates[:, :, None], axis=1))

    def one_expert(total, inputs):
        glu_w, linear_w, down_w, column = inputs
        act = clamped_unit(jnp.dot(normed, glu_w, preferred_element_type=jnp.float32), jnp.dot(normed, linear_w, preferred_element_type=jnp.float32)).astype(jnp.bfloat16)
        result = jnp.dot(act, down_w, preferred_element_type=jnp.float32)
        rounded = lax.optimization_barrier((result * column[:, None]).astype(jnp.bfloat16))
        return (total + rounded.astype(jnp.float32), None)
    mixture, _ = lax.scan(one_expert, jnp.zeros((SEQS, D), jnp.float32), (glu_weight, linear_weight, down_weight, share.T))
    combined = ALPHA * normed.astype(jnp.float32) + mixture
    layer_out = layer_norm(combined, final_gain).astype(jnp.bfloat16)
    return (layer_out, new_state)
```

```python
import functools

import jax
import jax.numpy as jnp
from jax import lax
from jax.experimental import pallas as pl
from jax.experimental.pallas import tpu as pltpu
from jax.sharding import PartitionSpec as P

ALPHA = 2.0**0.25
TAU = 16.0
LIMIT = 7.0
SLOPE = 1.702
EPSILON = 1e-05
MESH = pl.DeviceIdType.MESH
F32 = jnp.float32
BF16 = jnp.bfloat16
MIB = 1 << 20


def mm(a, b):
    return jnp.dot(a, b, preferred_element_type=F32)


def log_sigmoid(z):
    return jnp.minimum(z, 0.0) - jnp.log1p(jnp.exp(-jnp.abs(z)))


def project_kernel(
    tp, heads, dk, tokens, wq, wk, wv, dd, up, bias, pack_out, values_out,
    wq_v, wk_v, wv_v, dd_v, send, recv, load_sem, send_sem, recv_sem,
):
    me = lax.axis_index("tp")
    seqs, width = tokens.shape
    share = width // tp
    group = tp // heads
    loads = [
        pltpu.make_async_copy(src, dst, load_sem.at[i])
        for i, (src, dst) in enumerate(((wq, wq_v), (wk, wk_v), (wv, wv_v), (dd, dd_v)))
    ]
    for load in loads:
        load.start()
    barrier = pltpu.get_barrier_semaphore()

    @pl.loop(1, tp)
    def _(d):
        pl.semaphore_signal(
            barrier, inc=1, device_id={"tp": lax.rem(me + d, tp)}, device_id_type=MESH
        )

    own = tokens[:, pl.ds(pl.multiple_of(me * share, share), share)]
    for i, w in ((0, wq_v), (1, wk_v)):
        loads[i].wait()
        part = mm(own, w[...])
        for h in range(heads):
            send[h, i * seqs : (i + 1) * seqs, :] = part[:, h * dk : (h + 1) * dk].astype(BF16)
    pl.semaphore_wait(barrier, tp - 1)

    def copy_to(peer):
        return pltpu.make_async_remote_copy(
            src_ref=send.at[peer // group],
            dst_ref=recv.at[me],
            send_sem=send_sem.at[peer],
            recv_sem=recv_sem.at[me],
            device_id={"tp": peer},
            device_id_type=MESH,
        )

    def copy_from(peer):
        return pltpu.make_async_remote_copy(
            src_ref=send.at[0],
            dst_ref=recv.at[peer],
            send_sem=send_sem.at[peer],
            recv_sem=recv_sem.at[peer],
            device_id={"tp": peer},
            device_id_type=MESH,
        )

    @pl.loop(1, tp)
    def _(d):
        copy_to(lax.rem(me + d, tp)).start()

    head = me // group
    recv[me] = send[head]
    loads[2].wait()
    values_out[...] = mm(tokens[...], wv_v[...]).astype(BF16).astype(F32)
    loads[3].wait()
    low = mm(tokens[...], dd_v[...])
    cols = pl.ds(pl.multiple_of(head * dk, dk), dk)
    up_cols = up[:, cols]
    z = jnp.broadcast_to(bias[:, cols], (seqs, dk))
    for r in range(low.shape[1]):
        z = z + low[:, r : r + 1] * up_cols[r : r + 1, :]
    decay = jnp.exp(log_sigmoid(z) / TAU)

    @pl.loop(1, tp)
    def _(d):
        copy_from(lax.rem(me + d, tp)).wait_recv()

    total = recv[0].astype(F32)
    for p in range(1, tp):
        total = total + recv[p].astype(F32)
    total = total.astype(BF16).astype(F32)
    pad = pack_out.shape[1] - 3 * seqs
    pack = jnp.concatenate([decay, total, jnp.zeros((pad, dk), F32)], axis=0)
    pack_out[...] = jnp.transpose(pack)

    @pl.loop(1, tp)
    def _(d):
        copy_to(lax.rem(me + d, tp)).wait_send()


def state_kernel(pack, values, old, new, mixed, old_v, new_v, in_sem, out_sem):
    seqs, dk, dv = old_v.shape
    ins = [pltpu.make_async_copy(old.at[s], old_v.at[s], in_sem.at[s]) for s in range(seqs)]
    outs = [pltpu.make_async_copy(new_v.at[s], new.at[s], out_sem.at[s]) for s in range(seqs)]
    for s in range(seqs):
        ins[s].start()
    rows = []
    for s in range(seqs):
        ins[s].wait()
        value = values[s : s + 1, :]
        updated = pack[:, s : s + 1] * old_v[s] + pack[:, 2 * seqs + s : 2 * seqs + s + 1] * value
        new_v[s] = updated
        outs[s].start()
        rows.append(jnp.sum(pack[:, seqs + s : seqs + s + 1] * updated, axis=0, keepdims=True))
    mixed[...] = (jnp.concatenate(rows, axis=0) * dk ** (-0.5)).astype(BF16)
    for s in range(seqs):
        outs[s].wait()


def expert_kernel(
    ep, tp, tokens, mixed, gain, final_gain, routing, wo, router, wg, wl, wd, out,
    wo_v, router_v, wg_v, wl_v, wd_v, b_send, b_recv, rows, normed, d_send, d_recv, stats,
    load_sem, b_ss, b_rs, c_ss, c_rs, d_ss, d_rs, e_ss, e_rs,
):
    e = lax.axis_index("ep")
    t = lax.axis_index("tp")
    n = ep * tp
    me = e * tp + t
    seqs, width = tokens.shape
    share = width // tp
    experts = router_v.shape[1]
    loads = [
        pltpu.make_async_copy(src, dst, load_sem.at[i])
        for i, (src, dst) in enumerate(
            ((wo, wo_v), (wg.at[0], wg_v), (wl.at[0], wl_v), (router, router_v), (wd.at[0], wd_v))
        )
    ]
    for load in loads:
        load.start()
    barrier = pltpu.get_barrier_semaphore()

    def other(d):
        peer = lax.rem(me + d, n)
        return peer, peer // tp, lax.rem(peer, tp)

    @pl.loop(1, n)
    def _(d):
        _, pe, pt = other(d)
        pl.semaphore_signal(barrier, inc=1, device_id={"ep": pe, "tp": pt}, device_id_type=MESH)

    def remote(src, dst, ss, rs, pe, pt):
        return pltpu.make_async_remote_copy(
            src_ref=src, dst_ref=dst, send_sem=ss, recv_sem=rs,
            device_id={"ep": pe, "tp": pt}, device_id_type=MESH,
        )

    loads[0].wait()
    for p in range(tp):
        b_send[p] = mm(mixed[...], wo_v[:, p * share : (p + 1) * share]).astype(BF16)
    pl.semaphore_wait(barrier, n - 1)

    def b_out(p):
        return remote(b_send.at[p], b_recv.at[t], b_ss.at[p], b_rs.at[t], e, p)

    def b_in(p):
        return remote(b_send.at[p], b_recv.at[p], b_ss.at[p], b_rs.at[p], e, p)

    @pl.loop(1, tp)
    def _(d):
        b_out(lax.rem(t + d, tp)).start()

    b_recv[t] = b_send[t]
    share_cols = pl.ds(pl.multiple_of(t * share, share), share)
    hidden = ALPHA * tokens[:, share_cols].astype(F32)

    @pl.loop(1, tp)
    def _(d):
        b_in(lax.rem(t + d, tp)).wait_recv()

    for p in range(tp):
        hidden = hidden + b_recv[p].astype(F32)

    rows[t, e] = hidden.astype(rows.dtype)

    def c_out(d):
        peer, pe, pt = other(d)
        return remote(rows.at[t, e], rows.at[t, e], c_ss.at[peer], c_rs.at[me], pe, pt)

    def c_in(d):
        peer, pe, pt = other(d)
        return remote(rows.at[t, e], rows.at[pt, pe], c_ss.at[peer], c_rs.at[peer], pe, pt)

    @pl.loop(1, n)
    def _(d):
        c_out(d).start()

    @pl.loop(1, n)
    def _(d):
        c_in(d).wait_recv()

    total = jnp.zeros((ep * seqs, 1), F32)
    for p in range(tp):
        block = rows[p].reshape(ep * seqs, share).astype(F32)
        total = total + jnp.sum(block, axis=1, keepdims=True)
    mean = total / width
    square = jnp.zeros((ep * seqs, 1), F32)
    for p in range(tp):
        block = rows[p].reshape(ep * seqs, share).astype(F32) - mean
        square = square + jnp.sum(block * block, axis=1, keepdims=True)
    scale = lax.rsqrt(square / width + EPSILON)
    for i in (1, 2):
        loads[i].wait()
    glu = jnp.zeros((ep * seqs, wg_v.shape[1]), F32)
    linear = jnp.zeros((ep * seqs, wg_v.shape[1]), F32)
    for p in range(tp):
        block = rows[p].reshape(ep * seqs, share).astype(F32)
        block = ((block - mean) * scale * gain[:, p * share : (p + 1) * share]).astype(BF16)
        normed[p] = block.reshape(ep, seqs, share)
        glu = glu + mm(block, wg_v[p * share : (p + 1) * share, :])
        linear = linear + mm(block, wl_v[p * share : (p + 1) * share, :])
    glu = jnp.minimum(glu, LIMIT)
    linear = jnp.clip(linear, -LIMIT, LIMIT)
    act = (glu * jax.nn.sigmoid(SLOPE * glu) * (linear + 1.0)).astype(BF16)
    loads[4].wait()

    for p in range(tp):
        part = mm(act, wd_v[:, p * share : (p + 1) * share]).astype(BF16)
        d_send[p] = part.reshape(ep, seqs, share)

    def d_out(d):
        peer, pe, pt = other(d)
        return remote(d_send.at[pt, pe], d_recv.at[e, t], d_ss.at[peer], d_rs.at[me], pe, pt)

    def d_in(d):
        peer, pe, pt = other(d)
        return remote(d_send.at[pt, pe], d_recv.at[pe, pt], d_ss.at[peer], d_rs.at[peer], pe, pt)

    @pl.loop(1, n)
    def _(d):
        d_out(d).start()

    d_recv[e, t] = d_send[t, e]
    loads[3].wait()
    logits = jnp.zeros((seqs, experts), F32)
    for p in range(tp):
        logits = logits + mm(normed[p, e], router_v[p * share : (p + 1) * share, :])
    ids = lax.broadcasted_iota(jnp.int32, (seqs, experts), 1)
    routed = ids == routing[:, 0:1]
    for j in range(1, routing.shape[1]):
        routed = routed | (ids == routing[:, j : j + 1])
    top = jnp.max(jnp.where(routed, logits, -jnp.inf), axis=1, keepdims=True)
    raised = jnp.where(routed, jnp.exp(jnp.where(routed, logits - top, 0.0)), 0.0)
    gates = raised / jnp.sum(raised, axis=1, keepdims=True)
    combined = ALPHA * normed[t, e].astype(F32)

    @pl.loop(1, n)
    def _(d):
        d_in(d).wait_recv()

    for x in range(ep):
        summed = d_recv[x, 0].astype(F32)
        for p in range(1, tp):
            summed = summed + d_recv[x, p].astype(F32)
        combined = combined + (summed * gates[:, x : x + 1]).astype(BF16).astype(F32)

    own_sum = jnp.sum(combined, axis=1, keepdims=True)
    centred = combined - own_sum / share
    own_square = jnp.sum(centred * centred, axis=1, keepdims=True)
    lane = lax.broadcasted_iota(jnp.int32, stats.shape[1:], 1)
    stats[t] = jnp.where(lane == 0, own_sum, own_square)

    def e_out(p):
        return remote(stats.at[t], stats.at[t], e_ss.at[p], e_rs.at[t], e, p)

    def e_in(p):
        return remote(stats.at[t], stats.at[p], e_ss.at[p], e_rs.at[p], e, p)

    @pl.loop(1, tp)
    def _(d):
        e_out(lax.rem(t + d, tp)).start()

    @pl.loop(1, tp)
    def _(d):
        e_in(lax.rem(t + d, tp)).wait_recv()

    sums = [stats[p][:, 0:1] for p in range(tp)]
    mean = functools.reduce(jnp.add, sums) / width
    square = jnp.zeros((seqs, 1), F32)
    for p in range(tp):
        gap = sums[p] / share - mean
        square = square + stats[p][:, 1:2] + share * gap * gap
    scale = lax.rsqrt(square / width + EPSILON)
    out[...] = ((combined - mean) * scale * final_gain[:, share_cols]).astype(BF16)

    @pl.loop(1, tp)
    def _(d):
        b_out(lax.rem(t + d, tp)).wait_send()
        e_out(lax.rem(t + d, tp)).wait_send()

    @pl.loop(1, n)
    def _(d):
        c_out(d).wait_send()
        d_out(d).wait_send()


def per_device(
    tokens, query_weight, key_weight, value_weight, decay_down, decay_up, decay_bias, old_state,
    out_weight, norm_gain, router_weight, routing, glu_weight, linear_weight, down_weight,
    final_gain,
):
    tp = lax.axis_size("tp")
    ep = lax.axis_size("ep")
    n = ep * tp
    seqs, width = tokens.shape
    dk, dv = old_state.shape[1:]
    heads = query_weight.shape[1] // dk
    share = width // tp
    lanes = -(-3 * seqs // 128) * 128
    vmem = pl.BlockSpec(memory_space=pltpu.VMEM)
    hbm = pl.BlockSpec(memory_space=pl.ANY)
    dma = pltpu.SemaphoreType.DMA

    pack, values = pl.pallas_call(
        functools.partial(project_kernel, tp, heads, dk),
        out_shape=(
            jax.ShapeDtypeStruct((dk, lanes), F32),
            jax.ShapeDtypeStruct((seqs, dv), F32),
        ),
        in_specs=[vmem, hbm, hbm, hbm, hbm, vmem, vmem],
        out_specs=(vmem, vmem),
        scratch_shapes=[
            pltpu.VMEM(query_weight.shape, BF16),
            pltpu.VMEM(key_weight.shape, BF16),
            pltpu.VMEM(value_weight.shape, BF16),
            pltpu.VMEM(decay_down.shape, BF16),
            pltpu.VMEM((heads, 2 * seqs, dk), BF16),
            pltpu.VMEM((tp, 2 * seqs, dk), BF16),
            dma((4,)),
            dma((tp,)),
            dma((tp,)),
        ],
        compiler_params=pltpu.CompilerParams(
            collective_id=0, has_side_effects=True, vmem_limit_bytes=16 * MIB
        ),
        name="project",
    )(
        tokens, query_weight, key_weight, value_weight, decay_down, decay_up,
        decay_bias.reshape(1, -1),
    )

    new_state, mixed = pl.pallas_call(
        state_kernel,
        out_shape=(
            jax.ShapeDtypeStruct(old_state.shape, F32),
            jax.ShapeDtypeStruct((seqs, dv), BF16),
        ),
        in_specs=[vmem, vmem, hbm],
        out_specs=(hbm, vmem),
        scratch_shapes=[
            pltpu.VMEM(old_state.shape, F32),
            pltpu.VMEM(old_state.shape, F32),
            dma((seqs,)),
            dma((seqs,)),
        ],
        compiler_params=pltpu.CompilerParams(vmem_limit_bytes=24 * MIB),
        name="state",
    )(pack, values, old_state)

    layer_out = pl.pallas_call(
        functools.partial(expert_kernel, ep, tp),
        out_shape=jax.ShapeDtypeStruct((seqs, share), BF16),
        in_specs=[vmem] * 5 + [hbm] * 5,
        out_specs=vmem,
        scratch_shapes=[
            pltpu.VMEM(out_weight.shape, BF16),
            pltpu.VMEM(router_weight.shape, BF16),
            pltpu.VMEM(glu_weight.shape[1:], BF16),
            pltpu.VMEM(linear_weight.shape[1:], BF16),
            pltpu.VMEM(down_weight.shape[1:], BF16),
            pltpu.VMEM((tp, seqs, share), BF16),
            pltpu.VMEM((tp, seqs, share), BF16),
            pltpu.VMEM((tp, ep, seqs, share), BF16),
            pltpu.VMEM((tp, ep, seqs, share), BF16),
            pltpu.VMEM((tp, ep, seqs, share), BF16),
            pltpu.VMEM((ep, tp, seqs, share), BF16),
            pltpu.VMEM((tp, seqs, 128), F32),
            dma((5,)),
            dma((tp,)),
            dma((tp,)),
            dma((n,)),
            dma((n,)),
            dma((n,)),
            dma((n,)),
            dma((tp,)),
            dma((tp,)),
        ],
        compiler_params=pltpu.CompilerParams(
            collective_id=1, has_side_effects=True, vmem_limit_bytes=32 * MIB
        ),
        name="experts",
    )(
        tokens, mixed, norm_gain.reshape(1, -1), final_gain.reshape(1, -1), routing, out_weight,
        router_weight, glu_weight, linear_weight, down_weight,
    )
    return (layer_out, new_state)


def solution(mesh):
    return jax.shard_map(
        per_device,
        mesh=mesh,
        in_specs=(
            P("ep", None),
            P("tp", None),
            P("tp", None),
            P(None, "tp"),
            P(),
            P(),
            P(),
            P("ep", None, "tp"),
            P("tp", None),
            P(),
            P(),
            P("ep", None),
            P("ep", None, "tp"),
            P("ep", None, "tp"),
            P("ep", "tp", None),
            P(),
        ),
        out_specs=(P("ep", "tp"), P("ep", None, "tp")),
        check_vma=False,
    )
```

```python
import functools

import jax
import jax.numpy as jnp
from jax import lax
from jax.experimental import pallas as pl
from jax.experimental.pallas import tpu as pltpu
from jax.sharding import PartitionSpec as P

ALPHA = 2.0**0.25
TAU = 16.0
LIMIT = 7.0
SLOPE = 1.702
EPSILON = 1e-05
MESH = pl.DeviceIdType.MESH
F32 = jnp.float32
BF16 = jnp.bfloat16
MIB = 1 << 20


def mm(a, b):
    return jnp.dot(a, b, preferred_element_type=F32)


def log_sigmoid(z):
    return jnp.minimum(z, 0.0) - jnp.log1p(jnp.exp(-jnp.abs(z)))


def project_kernel(
    tp, heads, dk, tokens_h, wq, wk, wv, dd, up_h, bias_h, pack_out, values_out,
    tokens, wq_v, wk_v, wv_v, dd_v, up, bias, send, recv, load_sem, send_sem, recv_sem,
):
    me = lax.axis_index("tp")
    pairs = (
        (tokens_h, tokens), (wq, wq_v), (wk, wk_v), (dd, dd_v), (up_h, up), (bias_h, bias),
        (wv, wv_v),
    )
    loads = [
        pltpu.make_async_copy(src, dst, load_sem.at[i]) for i, (src, dst) in enumerate(pairs)
    ]
    for load in loads:
        load.start()
    seqs, width = tokens.shape
    share = width // tp
    group = tp // heads
    barrier = pltpu.get_barrier_semaphore()

    @pl.loop(1, tp)
    def _(d):
        pl.semaphore_signal(
            barrier, inc=1, device_id={"tp": lax.rem(me + d, tp)}, device_id_type=MESH
        )

    loads[0].wait()
    own = tokens[:, pl.ds(pl.multiple_of(me * share, share), share)]
    for i, w in ((0, wq_v), (1, wk_v)):
        loads[1 + i].wait()
        part = mm(own, w[...])
        for h in range(heads):
            send[h, i * seqs : (i + 1) * seqs, :] = part[:, h * dk : (h + 1) * dk].astype(BF16)
    pl.semaphore_wait(barrier, tp - 1)

    def copy_to(peer):
        return pltpu.make_async_remote_copy(
            src_ref=send.at[peer // group],
            dst_ref=recv.at[me],
            send_sem=send_sem.at[peer],
            recv_sem=recv_sem.at[me],
            device_id={"tp": peer},
            device_id_type=MESH,
        )

    def copy_from(peer):
        return pltpu.make_async_remote_copy(
            src_ref=send.at[0],
            dst_ref=recv.at[peer],
            send_sem=send_sem.at[peer],
            recv_sem=recv_sem.at[peer],
            device_id={"tp": peer},
            device_id_type=MESH,
        )

    @pl.loop(1, tp)
    def _(d):
        copy_to(lax.rem(me + d, tp)).start()

    head = me // group
    recv[me] = send[head]
    loads[3].wait()
    low = lax.dot_general(
        tokens[...], dd_v[...], (((1,), (1,)), ((), ())), preferred_element_type=F32
    )
    loads[4].wait()
    loads[5].wait()
    cols = pl.ds(pl.multiple_of(head * dk, dk), dk)
    up_cols = up[:, cols]
    z = jnp.broadcast_to(bias[:, cols], (seqs, dk))
    for r in range(low.shape[1]):
        z = z + low[:, r : r + 1] * up_cols[r : r + 1, :]
    decay = jnp.exp(log_sigmoid(z) / TAU)
    loads[6].wait()
    values_out[...] = mm(tokens[...], wv_v[...]).astype(BF16).astype(F32)

    @pl.loop(1, tp)
    def _(d):
        copy_from(lax.rem(me + d, tp)).wait_recv()

    total = recv[0].astype(F32)
    for p in range(1, tp):
        total = total + recv[p].astype(F32)
    total = total.astype(BF16).astype(F32)
    pad = pack_out.shape[1] - 3 * seqs
    pack = jnp.concatenate([decay, total, jnp.zeros((pad, dk), F32)], axis=0)
    pack_out[...] = jnp.transpose(pack)

    @pl.loop(1, tp)
    def _(d):
        copy_to(lax.rem(me + d, tp)).wait_send()


def state_kernel(pack, values, old, new, mixed, new_v, out_sem):
    seqs, dk, dv = old.shape
    outs = [pltpu.make_async_copy(new_v.at[s], new.at[s], out_sem.at[s]) for s in range(seqs)]
    rows = []
    for s in range(seqs):
        value = values[s : s + 1, :]
        updated = pack[:, s : s + 1] * old[s] + pack[:, 2 * seqs + s : 2 * seqs + s + 1] * value
        new_v[s] = updated
        outs[s].start()
        rows.append(jnp.sum(pack[:, seqs + s : seqs + s + 1] * updated, axis=0, keepdims=True))
    mixed[...] = (jnp.concatenate(rows, axis=0) * dk ** (-0.5)).astype(BF16)
    for s in range(seqs):
        outs[s].wait()


def expert_kernel(
    ep, tp, tokens, mixed, gain, final_gain, routing, router, wo, wg, wl, wd, out,
    wg_v, wl_v, wd_v, b_send, b_recv, rows, normed, own_part, pair_send, pair_recv,
    d_send, d_recv, f_send, f_recv, stats,
    load_sem, b_ss, b_rs, z_ss, x_ss, p_ss, c_rs, dp_ss, dp_rs, d_ss, d_rs, f_ss, f_rs, e_ss, e_rs,
):
    e = lax.axis_index("ep")
    t = lax.axis_index("tp")
    n = ep * tp
    me = e * tp + t
    zs = tp // 2
    zi = t // 2
    c = lax.rem(t, 2)
    mate = t + 1 - 2 * c
    seqs, width = tokens.shape
    share = width // tp
    loads = [
        pltpu.make_async_copy(src, dst, load_sem.at[i])
        for i, (src, dst) in enumerate(((wg.at[0], wg_v), (wl.at[0], wl_v), (wd.at[0], wd_v)))
    ]
    for load in loads:
        load.start()
    barrier = pltpu.get_barrier_semaphore()

    @pl.loop(1, n)
    def _(d):
        peer = lax.rem(me + d, n)
        pl.semaphore_signal(
            barrier, inc=1, device_id={"ep": peer // tp, "tp": lax.rem(peer, tp)},
            device_id_type=MESH,
        )

    def remote(src, dst, ss, rs, pe, pt):
        return pltpu.make_async_remote_copy(
            src_ref=src, dst_ref=dst, send_sem=ss, recv_sem=rs,
            device_id={"ep": pe, "tp": pt}, device_id_type=MESH,
        )

    for p in range(tp):
        b_send[p] = mm(mixed[...], wo[:, p * share : (p + 1) * share]).astype(BF16)
    pl.semaphore_wait(barrier, n - 1)

    def b_out(p):
        return remote(b_send.at[p], b_recv.at[t], b_ss.at[p], b_rs.at[t], e, p)

    def b_in(p):
        return remote(b_send.at[p], b_recv.at[p], b_ss.at[p], b_rs.at[p], e, p)

    @pl.loop(1, tp)
    def _(d):
        b_out(lax.rem(t + d, tp)).start()

    b_recv[t] = b_send[t]
    share_cols = pl.ds(pl.multiple_of(t * share, share), share)
    hidden = ALPHA * tokens[:, share_cols].astype(F32)

    @pl.loop(1, tp)
    def _(d):
        b_in(lax.rem(t + d, tp)).wait_recv()

    for p in range(tp):
        hidden = hidden + b_recv[p].astype(F32)

    rows[t, e] = hidden.astype(rows.dtype)

    def block(z, core, x):
        return rows.at[2 * z + core, x], c_rs.at[2 * z + core, x]

    def z_out(z):
        ref, sem = block(zi, c, e)
        return remote(ref, ref, z_ss.at[z], sem, e, 2 * z + c)

    def z_in(z):
        ref, sem = block(z, c, e)
        return remote(ref, ref, z_ss.at[z], sem, e, 2 * z + c)

    def x_out(z, x):
        ref, sem = block(z, c, e)
        return remote(ref, ref, x_ss.at[z, x], sem, x, t)

    def x_in(z, x):
        ref, sem = block(z, c, x)
        return remote(ref, ref, x_ss.at[z, x], sem, x, t)

    def p_out(z, x):
        ref, sem = block(z, c, x)
        return remote(ref, ref, p_ss.at[z, x], sem, e, mate)

    def p_in(z, x):
        ref, sem = block(z, 1 - c, x)
        return remote(ref, ref, p_ss.at[z, x], sem, e, mate)

    def around(i, d, size):
        return lax.rem(i + d, size)

    @pl.loop(1, zs)
    def _(d):
        z_out(around(zi, d, zs)).start()

    @pl.loop(0, zs)
    def _(d):
        z = around(zi, d, zs)

        @pl.when(d > 0)
        def _():
            z_in(z).wait_recv()

        @pl.loop(1, ep)
        def _(k):
            x_out(z, around(e, k, ep)).start()

        p_out(z, e).start()

    @pl.loop(0, zs)
    def _(d):
        z = around(zi, d, zs)

        @pl.loop(1, ep)
        def _(k):
            x = around(e, k, ep)
            x_in(z, x).wait_recv()
            p_out(z, x).start()

    @pl.loop(0, zs)
    def _(d):
        z = around(zi, d, zs)

        @pl.loop(0, ep)
        def _(k):
            p_in(z, around(e, k, ep)).wait_recv()

    total = jnp.zeros((ep * seqs, 1), F32)
    for p in range(tp):
        part = rows[p].reshape(ep * seqs, share).astype(F32)
        total = total + jnp.sum(part, axis=1, keepdims=True)
    mean = total / width
    square = jnp.zeros((ep * seqs, 1), F32)
    for p in range(tp):
        part = rows[p].reshape(ep * seqs, share).astype(F32) - mean
        square = square + jnp.sum(part * part, axis=1, keepdims=True)
    scale = lax.rsqrt(square / width + EPSILON)
    for i in (0, 1):
        loads[i].wait()
    glu = jnp.zeros((ep * seqs, wg_v.shape[1]), F32)
    linear = jnp.zeros((ep * seqs, wg_v.shape[1]), F32)
    for p in range(tp):
        part = rows[p].reshape(ep * seqs, share).astype(F32)
        part = ((part - mean) * scale * gain[:, p * share : (p + 1) * share]).astype(BF16)
        normed[p] = part.reshape(ep, seqs, share)
        glu = glu + mm(part, wg_v[p * share : (p + 1) * share, :])
        linear = linear + mm(part, wl_v[p * share : (p + 1) * share, :])
    glu = jnp.minimum(glu, LIMIT)
    linear = jnp.clip(linear, -LIMIT, LIMIT)
    act = (glu * jax.nn.sigmoid(SLOPE * glu) * (linear + 1.0)).astype(BF16)
    loads[2].wait()

    def down(z, core):
        first = pl.multiple_of((2 * z + core) * share, share)
        return mm(act, wd_v[:, pl.ds(first, share)])

    def pair_copy(z):
        return remote(pair_send.at[z], pair_recv.at[z], dp_ss.at[z], dp_rs.at[z], e, mate)

    def d_out(z, x):
        return remote(d_send.at[z, x], d_recv.at[z, e], d_ss.at[z, x], d_rs.at[z, e], x, t)

    def d_in(z, x):
        return remote(d_send.at[z, x], d_recv.at[z, x], d_ss.at[z, x], d_rs.at[z, x], x, t)

    def f_out(z):
        return remote(f_send.at[z], f_recv.at[zi], f_ss.at[z], f_rs.at[zi], e, 2 * z + c)

    def f_in(z):
        return remote(f_send.at[z], f_recv.at[z], f_ss.at[z], f_rs.at[z], e, 2 * z + c)

    for d in range(1, zs + 1):
        z = around(zi, d, zs)
        pair_send[z] = down(z, 1 - c).astype(BF16)
        pair_copy(z).start()
    for d in range(1, zs + 1):
        z = around(zi, d, zs)
        own_part[z] = down(z, c)

    @pl.loop(1, zs + 1)
    def _(d):
        z = around(zi, d, zs)
        pair_copy(z).wait_recv()
        both = (own_part[z] + pair_recv[z].astype(F32)).astype(BF16)
        d_send[z] = both.reshape(ep, seqs, share)

        @pl.loop(1, ep)
        def _(k):
            d_out(z, around(e, k, ep)).start()

        d_recv[z, e] = d_send[z, e]

    experts = router.shape[0]
    logits = jnp.zeros((experts, seqs), F32)
    for p in range(tp):
        logits = logits + lax.dot_general(
            router[:, p * share : (p + 1) * share], normed[p, e], (((1,), (1,)), ((), ())),
            preferred_element_type=F32,
        )
    ids = lax.broadcasted_iota(jnp.int32, (experts, seqs), 0)
    routed = ids == routing[0:1, :]
    for j in range(1, routing.shape[0]):
        routed = routed | (ids == routing[j : j + 1, :])
    top = jnp.max(jnp.where(routed, logits, -jnp.inf), axis=0, keepdims=True)
    raised = jnp.where(routed, jnp.exp(jnp.where(routed, logits - top, 0.0)), 0.0)
    gates = raised / jnp.sum(raised, axis=0, keepdims=True)
    tall, wide = -(-experts // 8) * 8, 128
    gates = jnp.concatenate([gates, jnp.zeros((experts, wide - seqs), F32)], axis=1)
    if tall > experts:
        gates = jnp.concatenate([gates, jnp.zeros((tall - experts, wide), F32)], axis=0)
    gates = jnp.transpose(gates)[:seqs, :]
    combined = ALPHA * normed[t, e].astype(F32)

    @pl.loop(1, zs + 1)
    def _(d):
        z = around(zi, d, zs)

        @pl.loop(1, ep)
        def _(k):
            d_in(z, around(e, k, ep)).wait_recv()

        summed = jnp.zeros((seqs, share), F32)
        for x in range(ep):
            summed = summed + d_recv[z, x].astype(F32) * gates[:, x : x + 1]
        f_send[z] = summed.astype(BF16)

        @pl.when(d < zs)
        def _():
            f_out(z).start()

    f_recv[zi] = f_send[zi]

    @pl.loop(1, zs)
    def _(d):
        f_in(around(zi, d, zs)).wait_recv()

    for z in range(zs):
        combined = combined + f_recv[z].astype(F32)

    own_sum = jnp.sum(combined, axis=1, keepdims=True)
    centred = combined - own_sum / share
    own_square = jnp.sum(centred * centred, axis=1, keepdims=True)
    lane = lax.broadcasted_iota(jnp.int32, stats.shape[1:], 1)
    stats[t] = jnp.where(lane == 0, own_sum, own_square)

    def e_out(p):
        return remote(stats.at[t], stats.at[t], e_ss.at[p], e_rs.at[t], e, p)

    def e_in(p):
        return remote(stats.at[t], stats.at[p], e_ss.at[p], e_rs.at[p], e, p)

    @pl.loop(1, tp)
    def _(d):
        e_out(lax.rem(t + d, tp)).start()

    @pl.loop(1, tp)
    def _(d):
        e_in(lax.rem(t + d, tp)).wait_recv()

    sums = [stats[p][:, 0:1] for p in range(tp)]
    mean = functools.reduce(jnp.add, sums) / width
    square = jnp.zeros((seqs, 1), F32)
    for p in range(tp):
        gap = sums[p] / share - mean
        square = square + stats[p][:, 1:2] + share * gap * gap
    scale = lax.rsqrt(square / width + EPSILON)
    out[...] = ((combined - mean) * scale * final_gain[:, share_cols]).astype(BF16)

    @pl.loop(1, tp)
    def _(d):
        b_out(lax.rem(t + d, tp)).wait_send()
        e_out(lax.rem(t + d, tp)).wait_send()

    @pl.loop(0, zs)
    def _(d):
        z = around(zi, d, zs)

        @pl.when(d > 0)
        def _():
            z_out(z).wait_send()
            f_out(z).wait_send()

        pair_copy(z).wait_send()

        @pl.loop(0, ep)
        def _(k):
            x = around(e, k, ep)
            p_out(z, x).wait_send()

            @pl.when(k > 0)
            def _():
                x_out(z, x).wait_send()
                d_out(z, x).wait_send()


def per_device(
    tokens, query_weight, key_weight, value_weight, decay_down, decay_up, decay_bias, old_state,
    out_weight, norm_gain, router_weight, routing, glu_weight, linear_weight, down_weight,
    final_gain,
):
    tp = lax.axis_size("tp")
    ep = lax.axis_size("ep")
    n = ep * tp
    seqs, width = tokens.shape
    dk, dv = old_state.shape[1:]
    heads = query_weight.shape[1] // dk
    share = width // tp
    lanes = -(-3 * seqs // 128) * 128
    vmem = pl.BlockSpec(memory_space=pltpu.VMEM)
    hbm = pl.BlockSpec(memory_space=pltpu.HBM)
    zs = tp // 2
    dma = pltpu.SemaphoreType.DMA

    pack, values = pl.pallas_call(
        functools.partial(project_kernel, tp, heads, dk),
        out_shape=(
            jax.ShapeDtypeStruct((dk, lanes), F32),
            jax.ShapeDtypeStruct((seqs, dv), F32),
        ),
        in_specs=[hbm] * 7,
        out_specs=(vmem, vmem),
        scratch_shapes=[
            pltpu.VMEM(tokens.shape, BF16),
            pltpu.VMEM(query_weight.shape, BF16),
            pltpu.VMEM(key_weight.shape, BF16),
            pltpu.VMEM(value_weight.shape, BF16),
            pltpu.VMEM(decay_down.shape[::-1], BF16),
            pltpu.VMEM(decay_up.shape, F32),
            pltpu.VMEM((1, decay_bias.shape[0]), F32),
            pltpu.VMEM((heads, 2 * seqs, dk), BF16),
            pltpu.VMEM((tp, 2 * seqs, dk), BF16),
            dma((7,)),
            dma((tp,)),
            dma((tp,)),
        ],
        compiler_params=pltpu.CompilerParams(
            collective_id=0, has_side_effects=True, vmem_limit_bytes=16 * MIB
        ),
        name="project",
    )(
        tokens, query_weight, key_weight, value_weight, decay_down.T, decay_up,
        decay_bias.reshape(1, -1),
    )

    new_state, mixed = pl.pallas_call(
        state_kernel,
        out_shape=(
            jax.ShapeDtypeStruct(old_state.shape, F32),
            jax.ShapeDtypeStruct((seqs, dv), BF16),
        ),
        in_specs=[vmem, vmem, vmem],
        out_specs=(hbm, vmem),
        scratch_shapes=[
            pltpu.VMEM(old_state.shape, F32),
            dma((seqs,)),
        ],
        compiler_params=pltpu.CompilerParams(vmem_limit_bytes=24 * MIB),
        name="state",
    )(pack, values, old_state)

    layer_out = pl.pallas_call(
        functools.partial(expert_kernel, ep, tp),
        out_shape=jax.ShapeDtypeStruct((seqs, share), BF16),
        in_specs=[vmem] * 7 + [hbm] * 3,
        out_specs=vmem,
        scratch_shapes=[
            pltpu.VMEM(glu_weight.shape[1:], BF16),
            pltpu.VMEM(linear_weight.shape[1:], BF16),
            pltpu.VMEM(down_weight.shape[1:], BF16),
            pltpu.VMEM((tp, seqs, share), BF16),
            pltpu.VMEM((tp, seqs, share), BF16),
            pltpu.VMEM((tp, ep, seqs, share), BF16),
            pltpu.VMEM((tp, ep, seqs, share), BF16),
            pltpu.VMEM((zs, ep * seqs, share), F32),
            pltpu.VMEM((zs, ep * seqs, share), BF16),
            pltpu.VMEM((zs, ep * seqs, share), BF16),
            pltpu.VMEM((zs, ep, seqs, share), BF16),
            pltpu.VMEM((zs, ep, seqs, share), BF16),
            pltpu.VMEM((zs, seqs, share), BF16),
            pltpu.VMEM((zs, seqs, share), BF16),
            pltpu.VMEM((tp, seqs, 128), F32),
            dma((3,)),
            dma((tp,)),
            dma((tp,)),
            dma((zs,)),
            dma((zs, ep)),
            dma((zs, ep)),
            dma((tp, ep)),
            dma((zs,)),
            dma((zs,)),
            dma((zs, ep)),
            dma((zs, ep)),
            dma((zs,)),
            dma((zs,)),
            dma((tp,)),
            dma((tp,)),
        ],
        compiler_params=pltpu.CompilerParams(
            collective_id=1, has_side_effects=True, vmem_limit_bytes=32 * MIB
        ),
        name="experts",
    )(
        tokens, mixed, norm_gain.reshape(1, -1), final_gain.reshape(1, -1), routing.T,
        router_weight.T, out_weight, glu_weight, linear_weight, down_weight,
    )
    return (layer_out, new_state)


def solution(mesh):
    return jax.shard_map(
        per_device,
        mesh=mesh,
        in_specs=(
            P("ep", None),
            P("tp", None),
            P("tp", None),
            P(None, "tp"),
            P(),
            P(),
            P(),
            P("ep", None, "tp"),
            P("tp", None),
            P(),
            P(),
            P("ep", None),
            P("ep", None, "tp"),
            P("ep", None, "tp"),
            P("ep", "tp", None),
            P(),
        ),
        out_specs=(P("ep", "tp"), P("ep", None, "tp")),
        check_vma=False,
    )
```

```python
import functools

import jax
import jax.numpy as jnp
from jax import lax
from jax.experimental import pallas as pl
from jax.experimental.pallas import tpu as pltpu
from jax.sharding import PartitionSpec as P

ALPHA = 2.0**0.25
TAU = 16.0
LIMIT = 7.0
SLOPE = 1.702
EPSILON = 1e-05
MESH = pl.DeviceIdType.MESH
F32 = jnp.float32
BF16 = jnp.bfloat16
MIB = 1 << 20


def mm(a, b):
    return jnp.dot(a, b, preferred_element_type=F32)


def log_sigmoid(z):
    return jnp.minimum(z, 0.0) - jnp.log1p(jnp.exp(-jnp.abs(z)))


def project_kernel(
    tp, heads, dk, tokens_h, wq, wk, wv, dd, up_h, bias_h, pack_out, values_out,
    tokens, wq_v, wk_v, wv_v, dd_v, up, bias, send, recv, load_sem, send_sem, recv_sem,
):
    me = lax.axis_index("tp")
    pairs = (
        (tokens_h, tokens), (wq, wq_v), (wk, wk_v), (dd, dd_v), (up_h, up), (bias_h, bias),
        (wv, wv_v),
    )
    loads = [
        pltpu.make_async_copy(src, dst, load_sem.at[i]) for i, (src, dst) in enumerate(pairs)
    ]
    for load in loads:
        load.start()
    seqs, width = tokens.shape
    share = width // tp
    group = tp // heads
    barrier = pltpu.get_barrier_semaphore()

    @pl.loop(1, tp)
    def _(d):
        pl.semaphore_signal(
            barrier, inc=1, device_id={"tp": lax.rem(me + d, tp)}, device_id_type=MESH
        )

    loads[0].wait()
    own = tokens[:, pl.ds(pl.multiple_of(me * share, share), share)]
    for i, w in ((0, wq_v), (1, wk_v)):
        loads[1 + i].wait()
        part = mm(own, w[...])
        for h in range(heads):
            send[h, i * seqs : (i + 1) * seqs, :] = part[:, h * dk : (h + 1) * dk].astype(BF16)
    pl.semaphore_wait(barrier, tp - 1)

    def copy_to(peer):
        return pltpu.make_async_remote_copy(
            src_ref=send.at[peer // group],
            dst_ref=recv.at[me],
            send_sem=send_sem.at[peer],
            recv_sem=recv_sem.at[me],
            device_id={"tp": peer},
            device_id_type=MESH,
        )

    def copy_from(peer):
        return pltpu.make_async_remote_copy(
            src_ref=send.at[0],
            dst_ref=recv.at[peer],
            send_sem=send_sem.at[peer],
            recv_sem=recv_sem.at[peer],
            device_id={"tp": peer},
            device_id_type=MESH,
        )

    @pl.loop(1, tp)
    def _(d):
        copy_to(lax.rem(me + d, tp)).start()

    head = me // group
    recv[me] = send[head]
    loads[3].wait()
    low = lax.dot_general(
        tokens[...], dd_v[...], (((1,), (1,)), ((), ())), preferred_element_type=F32
    )
    loads[4].wait()
    loads[5].wait()
    cols = pl.ds(pl.multiple_of(head * dk, dk), dk)
    up_cols = up[:, cols]
    z = jnp.broadcast_to(bias[:, cols], (seqs, dk))
    for r in range(low.shape[1]):
        z = z + low[:, r : r + 1] * up_cols[r : r + 1, :]
    decay = jnp.exp(log_sigmoid(z) / TAU)
    loads[6].wait()
    values_out[...] = mm(tokens[...], wv_v[...]).astype(BF16).astype(F32)

    @pl.loop(1, tp)
    def _(d):
        copy_from(lax.rem(me + d, tp)).wait_recv()

    total = recv[0].astype(F32)
    for p in range(1, tp):
        total = total + recv[p].astype(F32)
    total = total.astype(BF16).astype(F32)
    pad = pack_out.shape[1] - 3 * seqs
    pack = jnp.concatenate([decay, total, jnp.zeros((pad, dk), F32)], axis=0)
    pack_out[...] = jnp.transpose(pack)

    @pl.loop(1, tp)
    def _(d):
        copy_to(lax.rem(me + d, tp)).wait_send()


def state_kernel(pack, values, old, new, mixed, new_v, out_sem):
    seqs, dk, dv = old.shape
    outs = [pltpu.make_async_copy(new_v.at[s], new.at[s], out_sem.at[s]) for s in range(seqs)]
    rows = []
    for s in range(seqs):
        value = values[s : s + 1, :]
        updated = pack[:, s : s + 1] * old[s] + pack[:, 2 * seqs + s : 2 * seqs + s + 1] * value
        new_v[s] = updated
        outs[s].start()
        rows.append(jnp.sum(pack[:, seqs + s : seqs + s + 1] * updated, axis=0, keepdims=True))
    mixed[...] = (jnp.concatenate(rows, axis=0) * dk ** (-0.5)).astype(BF16)
    for s in range(seqs):
        outs[s].wait()


def expert_kernel(
    ep, tp, tokens, mixed, gain, final_gain, routing, router, wo, wg, wl, wd, out,
    wg_v, wl_v, wd_v, b_send, b_recv, rows, normed, own_part, pair_send, pair_recv,
    d_send, d_recv, f_send, f_recv, stats,
    load_sem, b_ss, b_rs, z_ss, x_ss, p_ss, c_rs, dp_ss, dp_rs, d_ss, d_rs, f_ss, f_rs, e_ss, e_rs,
):
    e = lax.axis_index("ep")
    t = lax.axis_index("tp")
    n = ep * tp
    me = e * tp + t
    zs = tp // 2
    zi = t // 2
    c = lax.rem(t, 2)
    mate = t + 1 - 2 * c
    seqs, width = tokens.shape
    share = width // tp
    loads = [
        pltpu.make_async_copy(src, dst, load_sem.at[i])
        for i, (src, dst) in enumerate(((wg.at[0], wg_v), (wl.at[0], wl_v), (wd.at[0], wd_v)))
    ]
    for load in loads:
        load.start()
    barrier = pltpu.get_barrier_semaphore()

    @pl.loop(1, n)
    def _(d):
        peer = lax.rem(me + d, n)
        pl.semaphore_signal(
            barrier, inc=1, device_id={"ep": peer // tp, "tp": lax.rem(peer, tp)},
            device_id_type=MESH,
        )

    def remote(src, dst, ss, rs, pe, pt):
        return pltpu.make_async_remote_copy(
            src_ref=src, dst_ref=dst, send_sem=ss, recv_sem=rs,
            device_id={"ep": pe, "tp": pt}, device_id_type=MESH,
        )

    for p in range(tp):
        b_send[p] = mm(mixed[...], wo[:, p * share : (p + 1) * share]).astype(BF16)
    pl.semaphore_wait(barrier, n - 1)

    def b_out(p):
        return remote(b_send.at[p], b_recv.at[t], b_ss.at[p], b_rs.at[t], e, p)

    def b_in(p):
        return remote(b_send.at[p], b_recv.at[p], b_ss.at[p], b_rs.at[p], e, p)

    @pl.loop(1, tp)
    def _(d):
        b_out(lax.rem(t + d, tp)).start()

    b_recv[t] = b_send[t]
    share_cols = pl.ds(pl.multiple_of(t * share, share), share)
    hidden = ALPHA * tokens[:, share_cols].astype(F32)

    @pl.loop(1, tp)
    def _(d):
        b_in(lax.rem(t + d, tp)).wait_recv()

    for p in range(tp):
        hidden = hidden + b_recv[p].astype(F32)

    rows[t, e] = hidden.astype(rows.dtype)

    def block(z, core, x):
        return rows.at[2 * z + core, x], c_rs.at[2 * z + core, x]

    def z_out(z):
        ref, sem = block(zi, c, e)
        return remote(ref, ref, z_ss.at[z], sem, e, 2 * z + c)

    def z_in(z):
        ref, sem = block(z, c, e)
        return remote(ref, ref, z_ss.at[z], sem, e, 2 * z + c)

    def x_out(z, x):
        ref, sem = block(z, c, e)
        return remote(ref, ref, x_ss.at[z, x], sem, x, t)

    def x_in(z, x):
        ref, sem = block(z, c, x)
        return remote(ref, ref, x_ss.at[z, x], sem, x, t)

    def p_out(z, x):
        ref, sem = block(z, c, x)
        return remote(ref, ref, p_ss.at[z, x], sem, e, mate)

    def p_in(z, x):
        ref, sem = block(z, 1 - c, x)
        return remote(ref, ref, p_ss.at[z, x], sem, e, mate)

    def around(i, d, size):
        return lax.rem(i + d, size)

    @pl.loop(1, zs)
    def _(d):
        z_out(around(zi, d, zs)).start()

    @pl.loop(0, zs)
    def _(d):
        z = around(zi, d, zs)

        @pl.when(d > 0)
        def _():
            z_in(z).wait_recv()

        @pl.loop(1, ep)
        def _(k):
            x_out(z, around(e, k, ep)).start()

        p_out(z, e).start()

    @pl.loop(0, zs)
    def _(d):
        z = around(zi, d, zs)

        @pl.loop(1, ep)
        def _(k):
            x = around(e, k, ep)
            x_in(z, x).wait_recv()
            p_out(z, x).start()

    @pl.loop(0, zs)
    def _(d):
        z = around(zi, d, zs)

        @pl.loop(0, ep)
        def _(k):
            p_in(z, around(e, k, ep)).wait_recv()

    total = jnp.zeros((ep * seqs, 1), F32)
    for p in range(tp):
        part = rows[p].reshape(ep * seqs, share).astype(F32)
        total = total + jnp.sum(part, axis=1, keepdims=True)
    mean = total / width
    square = jnp.zeros((ep * seqs, 1), F32)
    for p in range(tp):
        part = rows[p].reshape(ep * seqs, share).astype(F32) - mean
        square = square + jnp.sum(part * part, axis=1, keepdims=True)
    scale = lax.rsqrt(square / width + EPSILON)
    for i in (0, 1):
        loads[i].wait()
    glu = jnp.zeros((ep * seqs, wg_v.shape[1]), F32)
    linear = jnp.zeros((ep * seqs, wg_v.shape[1]), F32)
    for p in range(tp):
        part = rows[p].reshape(ep * seqs, share).astype(F32)
        part = ((part - mean) * scale * gain[:, p * share : (p + 1) * share]).astype(BF16)
        normed[p] = part.reshape(ep, seqs, share)
        glu = glu + mm(part, wg_v[p * share : (p + 1) * share, :])
        linear = linear + mm(part, wl_v[p * share : (p + 1) * share, :])
    glu = jnp.minimum(glu, LIMIT)
    linear = jnp.clip(linear, -LIMIT, LIMIT)
    act = (glu * jax.nn.sigmoid(SLOPE * glu) * (linear + 1.0)).astype(BF16)
    loads[2].wait()

    def down(z, core):
        first = pl.multiple_of((2 * z + core) * share, share)
        return mm(act, wd_v[:, pl.ds(first, share)])

    def pair_copy(z):
        return remote(pair_send.at[z], pair_recv.at[z], dp_ss.at[z], dp_rs.at[z], e, mate)

    def d_out(z, x):
        return remote(d_send.at[z, x], d_recv.at[z, e], d_ss.at[z, x], d_rs.at[z, e], x, t)

    def d_in(z, x):
        return remote(d_send.at[z, x], d_recv.at[z, x], d_ss.at[z, x], d_rs.at[z, x], x, t)

    def f_out(z):
        return remote(f_send.at[z], f_recv.at[zi], f_ss.at[z], f_rs.at[zi], e, 2 * z + c)

    def f_in(z):
        return remote(f_send.at[z], f_recv.at[z], f_ss.at[z], f_rs.at[z], e, 2 * z + c)

    for d in range(1, zs + 1):
        z = around(zi, d, zs)
        pair_send[z] = down(z, 1 - c).astype(BF16)
        pair_copy(z).start()
    for d in range(1, zs + 1):
        z = around(zi, d, zs)
        own_part[z] = down(z, c)

    @pl.loop(1, zs + 1)
    def _(d):
        z = around(zi, d, zs)
        pair_copy(z).wait_recv()
        both = (own_part[z] + pair_recv[z].astype(F32)).astype(BF16)
        d_send[z] = both.reshape(ep, seqs, share)

        @pl.loop(1, ep)
        def _(k):
            d_out(z, around(e, k, ep)).start()

        d_recv[z, e] = d_send[z, e]

    experts = router.shape[0]
    logits = jnp.zeros((experts, seqs), F32)
    for p in range(tp):
        logits = logits + lax.dot_general(
            router[:, p * share : (p + 1) * share], normed[p, e], (((1,), (1,)), ((), ())),
            preferred_element_type=F32,
        )
    ids = lax.broadcasted_iota(jnp.int32, (experts, seqs), 0)
    routed = ids == routing[0:1, :]
    for j in range(1, routing.shape[0]):
        routed = routed | (ids == routing[j : j + 1, :])
    top = jnp.max(jnp.where(routed, logits, -jnp.inf), axis=0, keepdims=True)
    raised = jnp.where(routed, jnp.exp(jnp.where(routed, logits - top, 0.0)), 0.0)
    gates = raised / jnp.sum(raised, axis=0, keepdims=True)
    tall, wide = -(-experts // 8) * 8, 128
    gates = jnp.concatenate([gates, jnp.zeros((experts, wide - seqs), F32)], axis=1)
    if tall > experts:
        gates = jnp.concatenate([gates, jnp.zeros((tall - experts, wide), F32)], axis=0)
    gates = jnp.transpose(gates)[:seqs, :]
    combined = ALPHA * normed[t, e].astype(F32)

    @pl.loop(1, zs + 1)
    def _(d):
        z = around(zi, d, zs)

        @pl.loop(1, ep)
        def _(k):
            d_in(z, around(e, k, ep)).wait_recv()

        summed = jnp.zeros((seqs, share), F32)
        for x in range(ep):
            summed = summed + d_recv[z, x].astype(F32) * gates[:, x : x + 1]
        f_send[z] = summed.astype(BF16)

        @pl.when(d < zs)
        def _():
            f_out(z).start()

    f_recv[zi] = f_send[zi]

    @pl.loop(1, zs)
    def _(d):
        f_in(around(zi, d, zs)).wait_recv()

    for z in range(zs):
        combined = combined + f_recv[z].astype(F32)

    own_sum = jnp.sum(combined, axis=1, keepdims=True)
    centred = combined - own_sum / share
    own_square = jnp.sum(centred * centred, axis=1, keepdims=True)
    lane = lax.broadcasted_iota(jnp.int32, stats.shape[1:], 1)
    stats[t] = jnp.where(lane == 0, own_sum, own_square)

    def e_out(p):
        return remote(stats.at[t], stats.at[t], e_ss.at[p], e_rs.at[t], e, p)

    def e_in(p):
        return remote(stats.at[t], stats.at[p], e_ss.at[p], e_rs.at[p], e, p)

    @pl.loop(1, tp)
    def _(d):
        e_out(lax.rem(t + d, tp)).start()

    @pl.loop(1, tp)
    def _(d):
        e_in(lax.rem(t + d, tp)).wait_recv()

    sums = [stats[p][:, 0:1] for p in range(tp)]
    mean = functools.reduce(jnp.add, sums) / width
    square = jnp.zeros((seqs, 1), F32)
    for p in range(tp):
        gap = sums[p] / share - mean
        square = square + stats[p][:, 1:2] + share * gap * gap
    scale = lax.rsqrt(square / width + EPSILON)
    out[...] = ((combined - mean) * scale * final_gain[:, share_cols]).astype(BF16)

    @pl.loop(1, tp)
    def _(d):
        b_out(lax.rem(t + d, tp)).wait_send()
        e_out(lax.rem(t + d, tp)).wait_send()

    @pl.loop(0, zs)
    def _(d):
        z = around(zi, d, zs)

        @pl.when(d > 0)
        def _():
            z_out(z).wait_send()
            f_out(z).wait_send()

        pair_copy(z).wait_send()

        @pl.loop(0, ep)
        def _(k):
            x = around(e, k, ep)
            p_out(z, x).wait_send()

            @pl.when(k > 0)
            def _():
                x_out(z, x).wait_send()
                d_out(z, x).wait_send()


def per_device(
    tokens, query_weight, key_weight, value_weight, decay_down, decay_up, decay_bias, old_state,
    out_weight, norm_gain, router_weight, routing, glu_weight, linear_weight, down_weight,
    final_gain,
):
    tp = lax.axis_size("tp")
    ep = lax.axis_size("ep")
    n = ep * tp
    seqs, width = tokens.shape
    dk, dv = old_state.shape[1:]
    heads = query_weight.shape[1] // dk
    share = width // tp
    lanes = -(-3 * seqs // 128) * 128
    vmem = pl.BlockSpec(memory_space=pltpu.VMEM)
    hbm = pl.BlockSpec(memory_space=pltpu.HBM)
    zs = tp // 2
    keep = lambda x: pltpu.with_memory_space_constraint(x, pltpu.HBM)
    dma = pltpu.SemaphoreType.DMA

    pack, values = pl.pallas_call(
        functools.partial(project_kernel, tp, heads, dk),
        out_shape=(
            jax.ShapeDtypeStruct((dk, lanes), F32),
            jax.ShapeDtypeStruct((seqs, dv), F32),
        ),
        in_specs=[hbm] * 7,
        out_specs=(vmem, vmem),
        scratch_shapes=[
            pltpu.VMEM(tokens.shape, BF16),
            pltpu.VMEM(query_weight.shape, BF16),
            pltpu.VMEM(key_weight.shape, BF16),
            pltpu.VMEM(value_weight.shape, BF16),
            pltpu.VMEM(decay_down.shape[::-1], BF16),
            pltpu.VMEM(decay_up.shape, F32),
            pltpu.VMEM((1, decay_bias.shape[0]), F32),
            pltpu.VMEM((heads, 2 * seqs, dk), BF16),
            pltpu.VMEM((tp, 2 * seqs, dk), BF16),
            dma((7,)),
            dma((tp,)),
            dma((tp,)),
        ],
        compiler_params=pltpu.CompilerParams(
            collective_id=0, has_side_effects=True, vmem_limit_bytes=16 * MIB
        ),
        name="project",
    )(
        keep(tokens), keep(query_weight), keep(key_weight), keep(value_weight),
        keep(decay_down.T), keep(decay_up), keep(decay_bias.reshape(1, -1)),
    )

    new_state, mixed = pl.pallas_call(
        state_kernel,
        out_shape=(
            jax.ShapeDtypeStruct(old_state.shape, F32),
            jax.ShapeDtypeStruct((seqs, dv), BF16),
        ),
        in_specs=[vmem, vmem, vmem],
        out_specs=(hbm, vmem),
        scratch_shapes=[
            pltpu.VMEM(old_state.shape, F32),
            dma((seqs,)),
        ],
        compiler_params=pltpu.CompilerParams(vmem_limit_bytes=24 * MIB),
        name="state",
    )(pack, values, old_state)

    layer_out = pl.pallas_call(
        functools.partial(expert_kernel, ep, tp),
        out_shape=jax.ShapeDtypeStruct((seqs, share), BF16),
        in_specs=[vmem] * 7 + [hbm] * 3,
        out_specs=vmem,
        scratch_shapes=[
            pltpu.VMEM(glu_weight.shape[1:], BF16),
            pltpu.VMEM(linear_weight.shape[1:], BF16),
            pltpu.VMEM(down_weight.shape[1:], BF16),
            pltpu.VMEM((tp, seqs, share), BF16),
            pltpu.VMEM((tp, seqs, share), BF16),
            pltpu.VMEM((tp, ep, seqs, share), BF16),
            pltpu.VMEM((tp, ep, seqs, share), BF16),
            pltpu.VMEM((zs, ep * seqs, share), F32),
            pltpu.VMEM((zs, ep * seqs, share), BF16),
            pltpu.VMEM((zs, ep * seqs, share), BF16),
            pltpu.VMEM((zs, ep, seqs, share), BF16),
            pltpu.VMEM((zs, ep, seqs, share), BF16),
            pltpu.VMEM((zs, seqs, share), BF16),
            pltpu.VMEM((zs, seqs, share), BF16),
            pltpu.VMEM((tp, seqs, 128), F32),
            dma((3,)),
            dma((tp,)),
            dma((tp,)),
            dma((zs,)),
            dma((zs, ep)),
            dma((zs, ep)),
            dma((tp, ep)),
            dma((zs,)),
            dma((zs,)),
            dma((zs, ep)),
            dma((zs, ep)),
            dma((zs,)),
            dma((zs,)),
            dma((tp,)),
            dma((tp,)),
        ],
        compiler_params=pltpu.CompilerParams(
            collective_id=1, has_side_effects=True, vmem_limit_bytes=32 * MIB
        ),
        name="experts",
    )(
        tokens, mixed, norm_gain.reshape(1, -1), final_gain.reshape(1, -1), routing.T,
        router_weight.T, out_weight, keep(glu_weight), keep(linear_weight), keep(down_weight),
    )
    return (layer_out, new_state)


def solution(mesh):
    return jax.shard_map(
        per_device,
        mesh=mesh,
        in_specs=(
            P("ep", None),
            P("tp", None),
            P("tp", None),
            P(None, "tp"),
            P(),
            P(),
            P(),
            P("ep", None, "tp"),
            P("tp", None),
            P(),
            P(),
            P("ep", None),
            P("ep", None, "tp"),
            P("ep", None, "tp"),
            P("ep", "tp", None),
            P(),
        ),
        out_specs=(P("ep", "tp"), P("ep", None, "tp")),
        check_vma=False,
    )
```

```python
import functools

import jax
import jax.numpy as jnp
from jax import lax
from jax.experimental import pallas as pl
from jax.experimental.pallas import tpu as pltpu
from jax.sharding import PartitionSpec as P

ALPHA = 2.0**0.25
TAU = 16.0
LIMIT = 7.0
SLOPE = 1.702
EPSILON = 1e-05
MESH = pl.DeviceIdType.MESH
F32 = jnp.float32
BF16 = jnp.bfloat16
MIB = 1 << 20


def mm(a, b):
    return jnp.dot(a, b, preferred_element_type=F32)


def log_sigmoid(z):
    return jnp.minimum(z, 0.0) - jnp.log1p(jnp.exp(-jnp.abs(z)))


def project_kernel(
    tp, heads, dk, tokens_h, wq, wk, wv, dd, up_h, bias_h, pack_out, values_out,
    tokens, wq_v, wk_v, wv_v, dd_v, up, bias, send, recv, load_sem, send_sem, recv_sem,
):
    me = lax.axis_index("tp")
    pairs = (
        (tokens_h, tokens), (wq, wq_v), (wk, wk_v), (dd, dd_v), (up_h, up), (bias_h, bias),
        (wv, wv_v),
    )
    loads = [
        pltpu.make_async_copy(src, dst, load_sem.at[i]) for i, (src, dst) in enumerate(pairs)
    ]
    for load in loads:
        load.start()
    seqs, width = tokens.shape
    share = width // tp
    group = tp // heads
    barrier = pltpu.get_barrier_semaphore()

    @pl.loop(1, tp)
    def _(d):
        pl.semaphore_signal(
            barrier, inc=1, device_id={"tp": lax.rem(me + d, tp)}, device_id_type=MESH
        )

    loads[0].wait()
    own = tokens[:, pl.ds(pl.multiple_of(me * share, share), share)]
    for i, w in ((0, wq_v), (1, wk_v)):
        loads[1 + i].wait()
        part = mm(own, w[...])
        for h in range(heads):
            send[h, i * seqs : (i + 1) * seqs, :] = part[:, h * dk : (h + 1) * dk].astype(BF16)
    pl.semaphore_wait(barrier, tp - 1)

    def copy_to(peer):
        return pltpu.make_async_remote_copy(
            src_ref=send.at[peer // group],
            dst_ref=recv.at[me],
            send_sem=send_sem.at[peer],
            recv_sem=recv_sem.at[me],
            device_id={"tp": peer},
            device_id_type=MESH,
        )

    def copy_from(peer):
        return pltpu.make_async_remote_copy(
            src_ref=send.at[0],
            dst_ref=recv.at[peer],
            send_sem=send_sem.at[peer],
            recv_sem=recv_sem.at[peer],
            device_id={"tp": peer},
            device_id_type=MESH,
        )

    @pl.loop(1, tp)
    def _(d):
        copy_to(lax.rem(me + d, tp)).start()

    head = me // group
    recv[me] = send[head]
    loads[3].wait()
    low = lax.dot_general(
        tokens[...], dd_v[...], (((1,), (1,)), ((), ())), preferred_element_type=F32
    )
    loads[4].wait()
    loads[5].wait()
    cols = pl.ds(pl.multiple_of(head * dk, dk), dk)
    up_cols = up[:, cols]
    z = jnp.broadcast_to(bias[:, cols], (seqs, dk))
    for r in range(low.shape[1]):
        z = z + low[:, r : r + 1] * up_cols[r : r + 1, :]
    decay = jnp.exp(log_sigmoid(z) / TAU)
    loads[6].wait()
    values_out[...] = mm(tokens[...], wv_v[...]).astype(BF16).astype(F32)

    @pl.loop(1, tp)
    def _(d):
        copy_from(lax.rem(me + d, tp)).wait_recv()

    total = recv[0].astype(F32)
    for p in range(1, tp):
        total = total + recv[p].astype(F32)
    total = total.astype(BF16).astype(F32)
    pad = pack_out.shape[1] - 3 * seqs
    pack = jnp.concatenate([decay, total, jnp.zeros((pad, dk), F32)], axis=0)
    pack_out[...] = jnp.transpose(pack)

    @pl.loop(1, tp)
    def _(d):
        copy_to(lax.rem(me + d, tp)).wait_send()


def state_kernel(pack, values, old, new, mixed, new_v, out_sem):
    seqs, dk, dv = old.shape
    outs = [pltpu.make_async_copy(new_v.at[s], new.at[s], out_sem.at[s]) for s in range(seqs)]
    rows = []
    for s in range(seqs):
        value = values[s : s + 1, :]
        updated = pack[:, s : s + 1] * old[s] + pack[:, 2 * seqs + s : 2 * seqs + s + 1] * value
        new_v[s] = updated
        outs[s].start()
        rows.append(jnp.sum(pack[:, seqs + s : seqs + s + 1] * updated, axis=0, keepdims=True))
    mixed[...] = (jnp.concatenate(rows, axis=0) * dk ** (-0.5)).astype(BF16)
    for s in range(seqs):
        outs[s].wait()


def expert_kernel(
    ep, tp, tokens, mixed, gain, final_gain, routing, router, wo, wg, wl, wd, out,
    wg_v, wl_v, wd_v, q_part, q_send, q_recv, b_send, b_recv, rows, normed, own_part, pair_send, pair_recv,
    d_send, d_recv, f_send, f_recv, stats,
    load_sem, q_ss, q_rs, b_ss, b_rs, z_ss, x_ss, p_ss, c_rs, dp_ss, dp_rs, d_ss, d_rs, f_ss, f_rs, e_ss, e_rs,
):
    e = lax.axis_index("ep")
    t = lax.axis_index("tp")
    zs = tp // 2
    zi = t // 2
    c = lax.rem(t, 2)
    mate = t + 1 - 2 * c
    seqs, width = tokens.shape
    share = width // tp
    loads = [
        pltpu.make_async_copy(src, dst, load_sem.at[i])
        for i, (src, dst) in enumerate(((wg.at[0], wg_v), (wl.at[0], wl_v), (wd.at[0], wd_v)))
    ]
    for load in loads:
        load.start()
    barrier = pltpu.get_barrier_semaphore()

    @pl.loop(1, tp)
    def _(d):
        pl.semaphore_signal(
            barrier, inc=1, device_id={"ep": e, "tp": lax.rem(t + d, tp)}, device_id_type=MESH
        )

    @pl.loop(1, ep)
    def _(d):
        pl.semaphore_signal(
            barrier, inc=1, device_id={"ep": lax.rem(e + d, ep), "tp": t}, device_id_type=MESH
        )

    def remote(src, dst, ss, rs, pe, pt):
        return pltpu.make_async_remote_copy(
            src_ref=src, dst_ref=dst, send_sem=ss, recv_sem=rs,
            device_id={"ep": pe, "tp": pt}, device_id_type=MESH,
        )

    def around(i, d, size):
        return lax.rem(i + d, size)

    def project(z, core):
        first = pl.multiple_of((2 * z + core) * share, share)
        return mm(mixed[...], wo[:, pl.ds(first, share)])

    def q_copy(z):
        return remote(q_send.at[z], q_recv.at[z], q_ss.at[z], q_rs.at[z], e, mate)

    def b_out(z):
        return remote(b_send.at[z], b_recv.at[zi], b_ss.at[z], b_rs.at[zi], e, 2 * z + c)

    def b_in(z):
        return remote(b_send.at[z], b_recv.at[z], b_ss.at[z], b_rs.at[z], e, 2 * z + c)

    for d in range(1, zs + 1):
        z = around(zi, d, zs)
        q_send[z] = project(z, 1 - c).astype(BF16)
    pl.semaphore_wait(barrier, tp + ep - 2)

    @pl.loop(1, zs + 1)
    def _(d):
        q_copy(around(zi, d, zs)).start()

    for d in range(1, zs + 1):
        z = around(zi, d, zs)
        q_part[z] = project(z, c)
    share_cols = pl.ds(pl.multiple_of(t * share, share), share)
    hidden = ALPHA * tokens[:, share_cols].astype(F32)

    @pl.loop(1, zs + 1)
    def _(d):
        z = around(zi, d, zs)
        q_copy(z).wait_recv()
        q_part[z] = q_part[z] + q_recv[z].astype(F32)

        @pl.when(d < zs)
        def _():
            b_send[z] = q_part[z].astype(BF16)
            b_out(z).start()

    hidden = hidden + q_part[zi]
    b_recv[zi] = jnp.zeros(b_recv.shape[1:], BF16)

    @pl.loop(1, zs)
    def _(d):
        b_in(around(zi, d, zs)).wait_recv()

    for z in range(zs):
        hidden = hidden + b_recv[z].astype(F32)

    rows[t, e] = hidden.astype(rows.dtype)

    def block(z, core, x):
        return rows.at[2 * z + core, x], c_rs.at[2 * z + core, x]

    def z_out(z):
        ref, sem = block(zi, c, e)
        return remote(ref, ref, z_ss.at[z], sem, e, 2 * z + c)

    def z_in(z):
        ref, sem = block(z, c, e)
        return remote(ref, ref, z_ss.at[z], sem, e, 2 * z + c)

    def x_out(z, x):
        ref, sem = block(z, c, e)
        return remote(ref, ref, x_ss.at[z, x], sem, x, t)

    def x_in(z, x):
        ref, sem = block(z, c, x)
        return remote(ref, ref, x_ss.at[z, x], sem, x, t)

    def p_out(z, x):
        ref, sem = block(z, c, x)
        return remote(ref, ref, p_ss.at[z, x], sem, e, mate)

    def p_in(z, x):
        ref, sem = block(z, 1 - c, x)
        return remote(ref, ref, p_ss.at[z, x], sem, e, mate)

    @pl.loop(1, zs)
    def _(d):
        z_out(around(zi, d, zs)).start()

    @pl.loop(0, zs)
    def _(d):
        z = around(zi, d, zs)

        @pl.when(d > 0)
        def _():
            z_in(z).wait_recv()

        @pl.loop(1, ep)
        def _(k):
            x_out(z, around(e, k, ep)).start()

        p_out(z, e).start()

    @pl.loop(0, zs)
    def _(d):
        z = around(zi, d, zs)

        @pl.loop(1, ep)
        def _(k):
            x = around(e, k, ep)
            x_in(z, x).wait_recv()
            p_out(z, x).start()

    @pl.loop(0, zs)
    def _(d):
        z = around(zi, d, zs)

        @pl.loop(0, ep)
        def _(k):
            p_in(z, around(e, k, ep)).wait_recv()

    total = jnp.zeros((ep * seqs, 1), F32)
    for p in range(tp):
        part = rows[p].reshape(ep * seqs, share).astype(F32)
        total = total + jnp.sum(part, axis=1, keepdims=True)
    mean = total / width
    square = jnp.zeros((ep * seqs, 1), F32)
    for p in range(tp):
        part = rows[p].reshape(ep * seqs, share).astype(F32) - mean
        square = square + jnp.sum(part * part, axis=1, keepdims=True)
    scale = lax.rsqrt(square / width + EPSILON)
    for i in (0, 1):
        loads[i].wait()
    glu = jnp.zeros((ep * seqs, wg_v.shape[1]), F32)
    linear = jnp.zeros((ep * seqs, wg_v.shape[1]), F32)
    for p in range(tp):
        part = rows[p].reshape(ep * seqs, share).astype(F32)
        part = ((part - mean) * scale * gain[:, p * share : (p + 1) * share]).astype(BF16)
        normed[p] = part.reshape(ep, seqs, share)
        glu = glu + mm(part, wg_v[p * share : (p + 1) * share, :])
        linear = linear + mm(part, wl_v[p * share : (p + 1) * share, :])
    glu = jnp.minimum(glu, LIMIT)
    linear = jnp.clip(linear, -LIMIT, LIMIT)
    act = (glu * jax.nn.sigmoid(SLOPE * glu) * (linear + 1.0)).astype(BF16)
    loads[2].wait()

    def down(z, core):
        first = pl.multiple_of((2 * z + core) * share, share)
        return mm(act, wd_v[:, pl.ds(first, share)])

    def pair_copy(z):
        return remote(pair_send.at[z], pair_recv.at[z], dp_ss.at[z], dp_rs.at[z], e, mate)

    def d_out(z, x):
        return remote(d_send.at[z, x], d_recv.at[z, e], d_ss.at[z, x], d_rs.at[z, e], x, t)

    def d_in(z, x):
        return remote(d_send.at[z, x], d_recv.at[z, x], d_ss.at[z, x], d_rs.at[z, x], x, t)

    def f_out(z):
        return remote(f_send.at[z], f_recv.at[zi], f_ss.at[z], f_rs.at[zi], e, 2 * z + c)

    def f_in(z):
        return remote(f_send.at[z], f_recv.at[z], f_ss.at[z], f_rs.at[z], e, 2 * z + c)

    for d in range(1, zs + 1):
        z = around(zi, d, zs)
        pair_send[z] = down(z, 1 - c).astype(BF16)
        pair_copy(z).start()
    for d in range(1, zs + 1):
        z = around(zi, d, zs)
        own_part[z] = down(z, c)

    @pl.loop(1, zs + 1)
    def _(d):
        z = around(zi, d, zs)
        pair_copy(z).wait_recv()
        both = (own_part[z] + pair_recv[z].astype(F32)).astype(BF16)
        d_send[z] = both.reshape(ep, seqs, share)

        @pl.loop(1, ep)
        def _(k):
            d_out(z, around(e, k, ep)).start()

        d_recv[z, e] = d_send[z, e]

    experts = router.shape[0]
    logits = jnp.zeros((experts, seqs), F32)
    for p in range(tp):
        logits = logits + lax.dot_general(
            router[:, p * share : (p + 1) * share], normed[p, e], (((1,), (1,)), ((), ())),
            preferred_element_type=F32,
        )
    ids = lax.broadcasted_iota(jnp.int32, (experts, seqs), 0)
    routed = ids == routing[0:1, :]
    for j in range(1, routing.shape[0]):
        routed = routed | (ids == routing[j : j + 1, :])
    top = jnp.max(jnp.where(routed, logits, -jnp.inf), axis=0, keepdims=True)
    raised = jnp.where(routed, jnp.exp(jnp.where(routed, logits - top, 0.0)), 0.0)
    gates = raised / jnp.sum(raised, axis=0, keepdims=True)
    tall, wide = -(-experts // 8) * 8, 128
    gates = jnp.concatenate([gates, jnp.zeros((experts, wide - seqs), F32)], axis=1)
    if tall > experts:
        gates = jnp.concatenate([gates, jnp.zeros((tall - experts, wide), F32)], axis=0)
    gates = jnp.transpose(gates)[:seqs, :]
    combined = ALPHA * normed[t, e].astype(F32)

    @pl.loop(1, zs + 1)
    def _(d):
        z = around(zi, d, zs)

        @pl.loop(1, ep)
        def _(k):
            d_in(z, around(e, k, ep)).wait_recv()

        summed = jnp.zeros((seqs, share), F32)
        for x in range(ep):
            summed = summed + d_recv[z, x].astype(F32) * gates[:, x : x + 1]
        f_send[z] = summed.astype(BF16)

        @pl.when(d < zs)
        def _():
            f_out(z).start()

    f_recv[zi] = f_send[zi]

    @pl.loop(1, zs)
    def _(d):
        f_in(around(zi, d, zs)).wait_recv()

    for z in range(zs):
        combined = combined + f_recv[z].astype(F32)

    own_sum = jnp.sum(combined, axis=1, keepdims=True)
    centred = combined - own_sum / share
    own_square = jnp.sum(centred * centred, axis=1, keepdims=True)
    lane = lax.broadcasted_iota(jnp.int32, (seqs, 128), 1)
    flat = jnp.transpose(jnp.where(lane == 0, own_sum, own_square))[0:2, :]
    stats[t] = jnp.concatenate([flat, jnp.zeros((2, 128 - seqs), F32)], axis=1)

    def e_out(p):
        return remote(stats.at[t], stats.at[t], e_ss.at[p], e_rs.at[t], e, p)

    def e_in(p):
        return remote(stats.at[t], stats.at[p], e_ss.at[p], e_rs.at[p], e, p)

    @pl.loop(1, tp)
    def _(d):
        e_out(lax.rem(t + d, tp)).start()

    @pl.loop(1, tp)
    def _(d):
        e_in(lax.rem(t + d, tp)).wait_recv()

    sums = [stats[p][0:1, :] for p in range(tp)]
    mean = functools.reduce(jnp.add, sums) / width
    square = jnp.zeros((1, 128), F32)
    for p in range(tp):
        gap = sums[p] / share - mean
        square = square + stats[p][1:2, :] + share * gap * gap
    scale = lax.rsqrt(square / width + EPSILON)
    row = lax.broadcasted_iota(jnp.int32, (8, 128), 0)
    tall = jnp.transpose(jnp.where(row == 0, mean, scale))
    mean, scale = tall[:seqs, 0:1], tall[:seqs, 1:2]
    out[...] = ((combined - mean) * scale * final_gain[:, share_cols]).astype(BF16)

    @pl.loop(1, tp)
    def _(d):
        e_out(lax.rem(t + d, tp)).wait_send()

    @pl.loop(0, zs)
    def _(d):
        z = around(zi, d, zs)

        @pl.when(d > 0)
        def _():
            b_out(z).wait_send()
            z_out(z).wait_send()
            f_out(z).wait_send()

        q_copy(z).wait_send()
        pair_copy(z).wait_send()

        @pl.loop(0, ep)
        def _(k):
            x = around(e, k, ep)
            p_out(z, x).wait_send()

            @pl.when(k > 0)
            def _():
                x_out(z, x).wait_send()
                d_out(z, x).wait_send()


def per_device(
    tokens, query_weight, key_weight, value_weight, decay_down, decay_up, decay_bias, old_state,
    out_weight, norm_gain, router_weight, routing, glu_weight, linear_weight, down_weight,
    final_gain,
):
    tp = lax.axis_size("tp")
    ep = lax.axis_size("ep")
    seqs, width = tokens.shape
    dk, dv = old_state.shape[1:]
    heads = query_weight.shape[1] // dk
    share = width // tp
    lanes = -(-3 * seqs // 128) * 128
    vmem = pl.BlockSpec(memory_space=pltpu.VMEM)
    hbm = pl.BlockSpec(memory_space=pltpu.HBM)
    zs = tp // 2
    keep = lambda x: pltpu.with_memory_space_constraint(x, pltpu.HBM)
    dma = pltpu.SemaphoreType.DMA

    pack, values = pl.pallas_call(
        functools.partial(project_kernel, tp, heads, dk),
        out_shape=(
            jax.ShapeDtypeStruct((dk, lanes), F32),
            jax.ShapeDtypeStruct((seqs, dv), F32),
        ),
        in_specs=[hbm] * 7,
        out_specs=(vmem, vmem),
        scratch_shapes=[
            pltpu.VMEM(tokens.shape, BF16),
            pltpu.VMEM(query_weight.shape, BF16),
            pltpu.VMEM(key_weight.shape, BF16),
            pltpu.VMEM(value_weight.shape, BF16),
            pltpu.VMEM(decay_down.shape[::-1], BF16),
            pltpu.VMEM(decay_up.shape, F32),
            pltpu.VMEM((1, decay_bias.shape[0]), F32),
            pltpu.VMEM((heads, 2 * seqs, dk), BF16),
            pltpu.VMEM((tp, 2 * seqs, dk), BF16),
            dma((7,)),
            dma((tp,)),
            dma((tp,)),
        ],
        compiler_params=pltpu.CompilerParams(
            collective_id=0, has_side_effects=True, vmem_limit_bytes=16 * MIB
        ),
        name="project",
    )(
        keep(tokens), keep(query_weight), keep(key_weight), keep(value_weight),
        keep(decay_down.T), keep(decay_up), keep(decay_bias.reshape(1, -1)),
    )

    new_state, mixed = pl.pallas_call(
        state_kernel,
        out_shape=(
            jax.ShapeDtypeStruct(old_state.shape, F32),
            jax.ShapeDtypeStruct((seqs, dv), BF16),
        ),
        in_specs=[vmem, vmem, vmem],
        out_specs=(hbm, vmem),
        scratch_shapes=[
            pltpu.VMEM(old_state.shape, F32),
            dma((seqs,)),
        ],
        compiler_params=pltpu.CompilerParams(vmem_limit_bytes=24 * MIB),
        name="state",
    )(pack, values, old_state)

    layer_out = pl.pallas_call(
        functools.partial(expert_kernel, ep, tp),
        out_shape=jax.ShapeDtypeStruct((seqs, share), BF16),
        in_specs=[vmem] * 7 + [hbm] * 3,
        out_specs=vmem,
        scratch_shapes=[
            pltpu.VMEM(glu_weight.shape[1:], BF16),
            pltpu.VMEM(linear_weight.shape[1:], BF16),
            pltpu.VMEM(down_weight.shape[1:], BF16),
            pltpu.VMEM((zs, seqs, share), F32),
            pltpu.VMEM((zs, seqs, share), BF16),
            pltpu.VMEM((zs, seqs, share), BF16),
            pltpu.VMEM((zs, seqs, share), BF16),
            pltpu.VMEM((zs, seqs, share), BF16),
            pltpu.VMEM((tp, ep, seqs, share), BF16),
            pltpu.VMEM((tp, ep, seqs, share), BF16),
            pltpu.VMEM((zs, ep * seqs, share), F32),
            pltpu.VMEM((zs, ep * seqs, share), BF16),
            pltpu.VMEM((zs, ep * seqs, share), BF16),
            pltpu.VMEM((zs, ep, seqs, share), BF16),
            pltpu.VMEM((zs, ep, seqs, share), BF16),
            pltpu.VMEM((zs, seqs, share), BF16),
            pltpu.VMEM((zs, seqs, share), BF16),
            pltpu.VMEM((tp, 2, 128), F32),
            dma((3,)),
            dma((zs,)),
            dma((zs,)),
            dma((zs,)),
            dma((zs,)),
            dma((zs,)),
            dma((zs, ep)),
            dma((zs, ep)),
            dma((tp, ep)),
            dma((zs,)),
            dma((zs,)),
            dma((zs, ep)),
            dma((zs, ep)),
            dma((zs,)),
            dma((zs,)),
            dma((tp,)),
            dma((tp,)),
        ],
        compiler_params=pltpu.CompilerParams(
            collective_id=1, has_side_effects=True, vmem_limit_bytes=32 * MIB
        ),
        name="experts",
    )(
        tokens, mixed, norm_gain.reshape(1, -1), final_gain.reshape(1, -1), routing.T,
        router_weight.T, out_weight, keep(glu_weight), keep(linear_weight), keep(down_weight),
    )
    return (layer_out, new_state)


def solution(mesh):
    return jax.shard_map(
        per_device,
        mesh=mesh,
        in_specs=(
            P("ep", None),
            P("tp", None),
            P("tp", None),
            P(None, "tp"),
            P(),
            P(),
            P(),
            P("ep", None, "tp"),
            P("tp", None),
            P(),
            P(),
            P("ep", None),
            P("ep", None, "tp"),
            P("ep", None, "tp"),
            P("ep", "tp", None),
            P(),
        ),
        out_specs=(P("ep", "tp"), P("ep", None, "tp")),
        check_vma=False,
    )
```

```python
import functools

import jax
import jax.numpy as jnp
from jax import lax
from jax.experimental import pallas as pl
from jax.experimental.pallas import tpu as pltpu
from jax.sharding import PartitionSpec as P

ALPHA = 2.0**0.25
TAU = 16.0
LIMIT = 7.0
SLOPE = 1.702
EPSILON = 1e-05
MESH = pl.DeviceIdType.MESH
F32 = jnp.float32
BF16 = jnp.bfloat16
MIB = 1 << 20


def mm(a, b):
    return jnp.dot(a, b, preferred_element_type=F32)


def log_sigmoid(z):
    return jnp.minimum(z, 0.0) - jnp.log1p(jnp.exp(-jnp.abs(z)))


def project_kernel(
    tp, heads, dk, tokens_h, wq, wk, wv, dd, up_h, bias_h, pack_out, values_out,
    tokens, wq_v, wk_v, wv_v, dd_v, up, bias, send, recv, load_sem, send_sem, recv_sem,
):
    me = lax.axis_index("tp")
    pairs = (
        (tokens_h, tokens), (wq, wq_v), (wk, wk_v), (dd, dd_v), (up_h, up), (bias_h, bias),
        (wv, wv_v),
    )
    loads = [
        pltpu.make_async_copy(src, dst, load_sem.at[i]) for i, (src, dst) in enumerate(pairs)
    ]
    for load in loads:
        load.start()
    seqs, width = tokens.shape
    share = width // tp
    group = tp // heads
    barrier = pltpu.get_barrier_semaphore()

    @pl.loop(1, tp, unroll=True)
    def _(d):
        pl.semaphore_signal(
            barrier, inc=1, device_id={"tp": lax.rem(me + d, tp)}, device_id_type=MESH
        )

    loads[0].wait()
    own = tokens[:, pl.ds(pl.multiple_of(me * share, share), share)]
    for i, w in ((0, wq_v), (1, wk_v)):
        loads[1 + i].wait()
        part = mm(own, w[...])
        for h in range(heads):
            send[h, i * seqs : (i + 1) * seqs, :] = part[:, h * dk : (h + 1) * dk].astype(BF16)
    pl.semaphore_wait(barrier, tp - 1)

    def copy_to(peer):
        return pltpu.make_async_remote_copy(
            src_ref=send.at[peer // group],
            dst_ref=recv.at[me],
            send_sem=send_sem.at[peer],
            recv_sem=recv_sem.at[me],
            device_id={"tp": peer},
            device_id_type=MESH,
        )

    def copy_from(peer):
        return pltpu.make_async_remote_copy(
            src_ref=send.at[0],
            dst_ref=recv.at[peer],
            send_sem=send_sem.at[peer],
            recv_sem=recv_sem.at[peer],
            device_id={"tp": peer},
            device_id_type=MESH,
        )

    @pl.loop(1, tp, unroll=True)
    def _(d):
        copy_to(lax.rem(me + d, tp)).start()

    head = me // group
    recv[me] = send[head]
    loads[3].wait()
    low = lax.dot_general(
        tokens[...], dd_v[...], (((1,), (1,)), ((), ())), preferred_element_type=F32
    )
    loads[4].wait()
    loads[5].wait()
    cols = pl.ds(pl.multiple_of(head * dk, dk), dk)
    up_cols = up[:, cols]
    z = jnp.broadcast_to(bias[:, cols], (seqs, dk))
    for r in range(low.shape[1]):
        z = z + low[:, r : r + 1] * up_cols[r : r + 1, :]
    decay = jnp.exp(log_sigmoid(z) / TAU)
    loads[6].wait()
    values_out[...] = mm(tokens[...], wv_v[...]).astype(BF16).astype(F32)

    @pl.loop(1, tp, unroll=True)
    def _(d):
        copy_from(lax.rem(me + d, tp)).wait_recv()

    total = recv[0].astype(F32)
    for p in range(1, tp):
        total = total + recv[p].astype(F32)
    total = total.astype(BF16).astype(F32)
    pad = pack_out.shape[1] - 3 * seqs
    pack = jnp.concatenate([decay, total, jnp.zeros((pad, dk), F32)], axis=0)
    pack_out[...] = jnp.transpose(pack)

    @pl.loop(1, tp, unroll=True)
    def _(d):
        copy_to(lax.rem(me + d, tp)).wait_send()


def state_kernel(pack, values, old, new, mixed, new_v, out_sem):
    seqs, dk, dv = old.shape
    outs = [pltpu.make_async_copy(new_v.at[s], new.at[s], out_sem.at[s]) for s in range(seqs)]
    rows = []
    for s in range(seqs):
        value = values[s : s + 1, :]
        updated = pack[:, s : s + 1] * old[s] + pack[:, 2 * seqs + s : 2 * seqs + s + 1] * value
        new_v[s] = updated
        outs[s].start()
        rows.append(jnp.sum(pack[:, seqs + s : seqs + s + 1] * updated, axis=0, keepdims=True))
    mixed[...] = (jnp.concatenate(rows, axis=0) * dk ** (-0.5)).astype(BF16)
    for s in range(seqs):
        outs[s].wait()


def expert_kernel(
    ep, tp, tokens, mixed, gain, final_gain, routing, router, wo, wg, wl, wd, out,
    wg_v, wl_v, wd_v, q_part, q_send, q_recv, b_send, b_recv, rows, normed, own_part, pair_send, pair_recv,
    d_send, d_recv, f_send, f_recv, stats,
    load_sem, q_ss, q_rs, b_ss, b_rs, z_ss, x_ss, p_ss, c_rs, dp_ss, dp_rs, d_ss, d_rs, f_ss, f_rs, e_ss, e_rs,
):
    e = lax.axis_index("ep")
    t = lax.axis_index("tp")
    zs = tp // 2
    zi = t // 2
    c = lax.rem(t, 2)
    mate = t + 1 - 2 * c
    seqs, width = tokens.shape
    share = width // tp
    loads = [
        pltpu.make_async_copy(src, dst, load_sem.at[i])
        for i, (src, dst) in enumerate(((wg.at[0], wg_v), (wl.at[0], wl_v), (wd.at[0], wd_v)))
    ]
    for load in loads:
        load.start()
    barrier = pltpu.get_barrier_semaphore()

    @pl.loop(1, tp, unroll=True)
    def _(d):
        pl.semaphore_signal(
            barrier, inc=1, device_id={"ep": e, "tp": lax.rem(t + d, tp)}, device_id_type=MESH
        )

    @pl.loop(1, ep, unroll=True)
    def _(d):
        pl.semaphore_signal(
            barrier, inc=1, device_id={"ep": lax.rem(e + d, ep), "tp": t}, device_id_type=MESH
        )

    def remote(src, dst, ss, rs, pe, pt):
        return pltpu.make_async_remote_copy(
            src_ref=src, dst_ref=dst, send_sem=ss, recv_sem=rs,
            device_id={"ep": pe, "tp": pt}, device_id_type=MESH,
        )

    def around(i, d, size):
        return lax.rem(i + d, size)

    def project(z, core):
        first = pl.multiple_of((2 * z + core) * share, share)
        return mm(mixed[...], wo[:, pl.ds(first, share)])

    def q_copy(z):
        return remote(q_send.at[z], q_recv.at[z], q_ss.at[z], q_rs.at[z], e, mate)

    def b_out(z):
        return remote(b_send.at[z], b_recv.at[zi], b_ss.at[z], b_rs.at[zi], e, 2 * z + c)

    def b_in(z):
        return remote(b_send.at[z], b_recv.at[z], b_ss.at[z], b_rs.at[z], e, 2 * z + c)

    for d in range(1, zs + 1):
        z = around(zi, d, zs)
        q_send[z] = project(z, 1 - c).astype(BF16)
    pl.semaphore_wait(barrier, tp + ep - 2)

    @pl.loop(1, zs + 1, unroll=True)
    def _(d):
        q_copy(around(zi, d, zs)).start()

    for d in range(1, zs + 1):
        z = around(zi, d, zs)
        q_part[z] = project(z, c)
    share_cols = pl.ds(pl.multiple_of(t * share, share), share)
    hidden = ALPHA * tokens[:, share_cols].astype(F32)

    @pl.loop(1, zs + 1, unroll=True)
    def _(d):
        z = around(zi, d, zs)
        q_copy(z).wait_recv()
        q_part[z] = q_part[z] + q_recv[z].astype(F32)

        @pl.when(d < zs)
        def _():
            b_send[z] = q_part[z].astype(BF16)
            b_out(z).start()

    hidden = hidden + q_part[zi]
    b_recv[zi] = jnp.zeros(b_recv.shape[1:], BF16)

    @pl.loop(1, zs, unroll=True)
    def _(d):
        b_in(around(zi, d, zs)).wait_recv()

    for z in range(zs):
        hidden = hidden + b_recv[z].astype(F32)

    rows[t, e] = hidden.astype(rows.dtype)

    def block(z, core, x):
        return rows.at[2 * z + core, x], c_rs.at[2 * z + core, x]

    def z_out(z):
        ref, sem = block(zi, c, e)
        return remote(ref, ref, z_ss.at[z], sem, e, 2 * z + c)

    def z_in(z):
        ref, sem = block(z, c, e)
        return remote(ref, ref, z_ss.at[z], sem, e, 2 * z + c)

    def x_out(z, x):
        ref, sem = block(z, c, e)
        return remote(ref, ref, x_ss.at[z, x], sem, x, t)

    def x_in(z, x):
        ref, sem = block(z, c, x)
        return remote(ref, ref, x_ss.at[z, x], sem, x, t)

    def p_out(z, x):
        ref, sem = block(z, c, x)
        return remote(ref, ref, p_ss.at[z, x], sem, e, mate)

    def p_in(z, x):
        ref, sem = block(z, 1 - c, x)
        return remote(ref, ref, p_ss.at[z, x], sem, e, mate)

    @pl.loop(1, zs, unroll=True)
    def _(d):
        z_out(around(zi, d, zs)).start()

    @pl.loop(0, zs, unroll=True)
    def _(d):
        z = around(zi, d, zs)

        @pl.when(d > 0)
        def _():
            z_in(z).wait_recv()

        @pl.loop(1, ep, unroll=True)
        def _(k):
            x_out(z, around(e, k, ep)).start()

        p_out(z, e).start()

    @pl.loop(0, zs, unroll=True)
    def _(d):
        z = around(zi, d, zs)

        @pl.loop(1, ep, unroll=True)
        def _(k):
            x = around(e, k, ep)
            x_in(z, x).wait_recv()
            p_out(z, x).start()

    @pl.loop(0, zs, unroll=True)
    def _(d):
        z = around(zi, d, zs)

        @pl.loop(0, ep, unroll=True)
        def _(k):
            p_in(z, around(e, k, ep)).wait_recv()

    total = jnp.zeros((ep * seqs, 1), F32)
    for p in range(tp):
        part = rows[p].reshape(ep * seqs, share).astype(F32)
        total = total + jnp.sum(part, axis=1, keepdims=True)
    mean = total / width
    square = jnp.zeros((ep * seqs, 1), F32)
    for p in range(tp):
        part = rows[p].reshape(ep * seqs, share).astype(F32) - mean
        square = square + jnp.sum(part * part, axis=1, keepdims=True)
    scale = lax.rsqrt(square / width + EPSILON)
    for i in (0, 1):
        loads[i].wait()
    glu = jnp.zeros((ep * seqs, wg_v.shape[1]), F32)
    linear = jnp.zeros((ep * seqs, wg_v.shape[1]), F32)
    for p in range(tp):
        part = rows[p].reshape(ep * seqs, share).astype(F32)
        part = ((part - mean) * scale * gain[:, p * share : (p + 1) * share]).astype(BF16)
        normed[p] = part.reshape(ep, seqs, share)
        glu = glu + mm(part, wg_v[p * share : (p + 1) * share, :])
        linear = linear + mm(part, wl_v[p * share : (p + 1) * share, :])
    glu = jnp.minimum(glu, LIMIT)
    linear = jnp.clip(linear, -LIMIT, LIMIT)
    act = (glu * jax.nn.sigmoid(SLOPE * glu) * (linear + 1.0)).astype(BF16)
    loads[2].wait()

    def down(z, core):
        first = pl.multiple_of((2 * z + core) * share, share)
        return mm(act, wd_v[:, pl.ds(first, share)])

    def pair_copy(z):
        return remote(pair_send.at[z], pair_recv.at[z], dp_ss.at[z], dp_rs.at[z], e, mate)

    def d_out(z, x):
        return remote(d_send.at[z, x], d_recv.at[z, e], d_ss.at[z, x], d_rs.at[z, e], x, t)

    def d_in(z, x):
        return remote(d_send.at[z, x], d_recv.at[z, x], d_ss.at[z, x], d_rs.at[z, x], x, t)

    def f_out(z):
        return remote(f_send.at[z], f_recv.at[zi], f_ss.at[z], f_rs.at[zi], e, 2 * z + c)

    def f_in(z):
        return remote(f_send.at[z], f_recv.at[z], f_ss.at[z], f_rs.at[z], e, 2 * z + c)

    for d in range(1, zs + 1):
        z = around(zi, d, zs)
        pair_send[z] = down(z, 1 - c).astype(BF16)
        pair_copy(z).start()
    for d in range(1, zs + 1):
        z = around(zi, d, zs)
        own_part[z] = down(z, c)

    @pl.loop(1, zs + 1, unroll=True)
    def _(d):
        z = around(zi, d, zs)
        pair_copy(z).wait_recv()
        both = (own_part[z] + pair_recv[z].astype(F32)).astype(BF16)
        d_send[z] = both.reshape(ep, seqs, share)

        @pl.loop(1, ep, unroll=True)
        def _(k):
            d_out(z, around(e, k, ep)).start()

        d_recv[z, e] = d_send[z, e]

    experts = router.shape[0]
    logits = jnp.zeros((experts, seqs), F32)
    for p in range(tp):
        logits = logits + lax.dot_general(
            router[:, p * share : (p + 1) * share], normed[p, e], (((1,), (1,)), ((), ())),
            preferred_element_type=F32,
        )
    ids = lax.broadcasted_iota(jnp.int32, (experts, seqs), 0)
    routed = ids == routing[0:1, :]
    for j in range(1, routing.shape[0]):
        routed = routed | (ids == routing[j : j + 1, :])
    top = jnp.max(jnp.where(routed, logits, -jnp.inf), axis=0, keepdims=True)
    raised = jnp.where(routed, jnp.exp(jnp.where(routed, logits - top, 0.0)), 0.0)
    gates = raised / jnp.sum(raised, axis=0, keepdims=True)
    tall, wide = -(-experts // 8) * 8, 128
    gates = jnp.concatenate([gates, jnp.zeros((experts, wide - seqs), F32)], axis=1)
    if tall > experts:
        gates = jnp.concatenate([gates, jnp.zeros((tall - experts, wide), F32)], axis=0)
    gates = jnp.transpose(gates)[:seqs, :]
    combined = ALPHA * normed[t, e].astype(F32)

    @pl.loop(1, zs + 1, unroll=True)
    def _(d):
        z = around(zi, d, zs)

        @pl.loop(1, ep, unroll=True)
        def _(k):
            d_in(z, around(e, k, ep)).wait_recv()

        summed = jnp.zeros((seqs, share), F32)
        for x in range(ep):
            summed = summed + d_recv[z, x].astype(F32) * gates[:, x : x + 1]
        f_send[z] = summed.astype(BF16)

        @pl.when(d < zs)
        def _():
            f_out(z).start()

    f_recv[zi] = f_send[zi]

    @pl.loop(1, zs, unroll=True)
    def _(d):
        f_in(around(zi, d, zs)).wait_recv()

    for z in range(zs):
        combined = combined + f_recv[z].astype(F32)

    own_sum = jnp.sum(combined, axis=1, keepdims=True)
    centred = combined - own_sum / share
    own_square = jnp.sum(centred * centred, axis=1, keepdims=True)
    lane = lax.broadcasted_iota(jnp.int32, (seqs, 128), 1)
    flat = jnp.transpose(jnp.where(lane == 0, own_sum, own_square))[0:2, :]
    stats[t] = jnp.concatenate([flat, jnp.zeros((2, 128 - seqs), F32)], axis=1)

    def e_out(p):
        return remote(stats.at[t], stats.at[t], e_ss.at[p], e_rs.at[t], e, p)

    def e_in(p):
        return remote(stats.at[t], stats.at[p], e_ss.at[p], e_rs.at[p], e, p)

    @pl.loop(1, tp, unroll=True)
    def _(d):
        e_out(lax.rem(t + d, tp)).start()

    @pl.loop(1, tp, unroll=True)
    def _(d):
        e_in(lax.rem(t + d, tp)).wait_recv()

    sums = [stats[p][0:1, :] for p in range(tp)]
    mean = functools.reduce(jnp.add, sums) / width
    square = jnp.zeros((1, 128), F32)
    for p in range(tp):
        gap = sums[p] / share - mean
        square = square + stats[p][1:2, :] + share * gap * gap
    scale = lax.rsqrt(square / width + EPSILON)
    row = lax.broadcasted_iota(jnp.int32, (8, 128), 0)
    tall = jnp.transpose(jnp.where(row == 0, mean, scale))
    mean, scale = tall[:seqs, 0:1], tall[:seqs, 1:2]
    out[...] = ((combined - mean) * scale * final_gain[:, share_cols]).astype(BF16)

    @pl.loop(1, tp, unroll=True)
    def _(d):
        e_out(lax.rem(t + d, tp)).wait_send()

    @pl.loop(0, zs, unroll=True)
    def _(d):
        z = around(zi, d, zs)

        @pl.when(d > 0)
        def _():
            b_out(z).wait_send()
            z_out(z).wait_send()
            f_out(z).wait_send()

        q_copy(z).wait_send()
        pair_copy(z).wait_send()

        @pl.loop(0, ep, unroll=True)
        def _(k):
            x = around(e, k, ep)
            p_out(z, x).wait_send()

            @pl.when(k > 0)
            def _():
                x_out(z, x).wait_send()
                d_out(z, x).wait_send()


def per_device(
    tokens, query_weight, key_weight, value_weight, decay_down, decay_up, decay_bias, old_state,
    out_weight, norm_gain, router_weight, routing, glu_weight, linear_weight, down_weight,
    final_gain,
):
    tp = lax.axis_size("tp")
    ep = lax.axis_size("ep")
    seqs, width = tokens.shape
    dk, dv = old_state.shape[1:]
    heads = query_weight.shape[1] // dk
    share = width // tp
    lanes = -(-3 * seqs // 128) * 128
    vmem = pl.BlockSpec(memory_space=pltpu.VMEM)
    hbm = pl.BlockSpec(memory_space=pltpu.HBM)
    zs = tp // 2
    keep = lambda x: pltpu.with_memory_space_constraint(x, pltpu.HBM)
    dma = pltpu.SemaphoreType.DMA

    pack, values = pl.pallas_call(
        functools.partial(project_kernel, tp, heads, dk),
        out_shape=(
            jax.ShapeDtypeStruct((dk, lanes), F32),
            jax.ShapeDtypeStruct((seqs, dv), F32),
        ),
        in_specs=[hbm] * 7,
        out_specs=(vmem, vmem),
        scratch_shapes=[
            pltpu.VMEM(tokens.shape, BF16),
            pltpu.VMEM(query_weight.shape, BF16),
            pltpu.VMEM(key_weight.shape, BF16),
            pltpu.VMEM(value_weight.shape, BF16),
            pltpu.VMEM(decay_down.shape[::-1], BF16),
            pltpu.VMEM(decay_up.shape, F32),
            pltpu.VMEM((1, decay_bias.shape[0]), F32),
            pltpu.VMEM((heads, 2 * seqs, dk), BF16),
            pltpu.VMEM((tp, 2 * seqs, dk), BF16),
            dma((7,)),
            dma((tp,)),
            dma((tp,)),
        ],
        compiler_params=pltpu.CompilerParams(
            collective_id=0, has_side_effects=True, vmem_limit_bytes=16 * MIB
        ),
        name="project",
    )(
        keep(tokens), keep(query_weight), keep(key_weight), keep(value_weight),
        keep(decay_down.T), keep(decay_up), keep(decay_bias.reshape(1, -1)),
    )

    new_state, mixed = pl.pallas_call(
        state_kernel,
        out_shape=(
            jax.ShapeDtypeStruct(old_state.shape, F32),
            jax.ShapeDtypeStruct((seqs, dv), BF16),
        ),
        in_specs=[vmem, vmem, vmem],
        out_specs=(hbm, vmem),
        scratch_shapes=[
            pltpu.VMEM(old_state.shape, F32),
            dma((seqs,)),
        ],
        compiler_params=pltpu.CompilerParams(vmem_limit_bytes=24 * MIB),
        name="state",
    )(pack, values, old_state)

    layer_out = pl.pallas_call(
        functools.partial(expert_kernel, ep, tp),
        out_shape=jax.ShapeDtypeStruct((seqs, share), BF16),
        in_specs=[vmem] * 7 + [hbm] * 3,
        out_specs=vmem,
        scratch_shapes=[
            pltpu.VMEM(glu_weight.shape[1:], BF16),
            pltpu.VMEM(linear_weight.shape[1:], BF16),
            pltpu.VMEM(down_weight.shape[1:], BF16),
            pltpu.VMEM((zs, seqs, share), F32),
            pltpu.VMEM((zs, seqs, share), BF16),
            pltpu.VMEM((zs, seqs, share), BF16),
            pltpu.VMEM((zs, seqs, share), BF16),
            pltpu.VMEM((zs, seqs, share), BF16),
            pltpu.VMEM((tp, ep, seqs, share), BF16),
            pltpu.VMEM((tp, ep, seqs, share), BF16),
            pltpu.VMEM((zs, ep * seqs, share), F32),
            pltpu.VMEM((zs, ep * seqs, share), BF16),
            pltpu.VMEM((zs, ep * seqs, share), BF16),
            pltpu.VMEM((zs, ep, seqs, share), BF16),
            pltpu.VMEM((zs, ep, seqs, share), BF16),
            pltpu.VMEM((zs, seqs, share), BF16),
            pltpu.VMEM((zs, seqs, share), BF16),
            pltpu.VMEM((tp, 2, 128), F32),
            dma((3,)),
            dma((zs,)),
            dma((zs,)),
            dma((zs,)),
            dma((zs,)),
            dma((zs,)),
            dma((zs, ep)),
            dma((zs, ep)),
            dma((tp, ep)),
            dma((zs,)),
            dma((zs,)),
            dma((zs, ep)),
            dma((zs, ep)),
            dma((zs,)),
            dma((zs,)),
            dma((tp,)),
            dma((tp,)),
        ],
        compiler_params=pltpu.CompilerParams(
            collective_id=1, has_side_effects=True, vmem_limit_bytes=32 * MIB
        ),
        name="experts",
    )(
        tokens, mixed, norm_gain.reshape(1, -1), final_gain.reshape(1, -1), routing.T,
        router_weight.T, out_weight, keep(glu_weight), keep(linear_weight), keep(down_weight),
    )
    return (layer_out, new_state)


def solution(mesh):
    return jax.shard_map(
        per_device,
        mesh=mesh,
        in_specs=(
            P("ep", None),
            P("tp", None),
            P("tp", None),
            P(None, "tp"),
            P(),
            P(),
            P(),
            P("ep", None, "tp"),
            P("tp", None),
            P(),
            P(),
            P("ep", None),
            P("ep", None, "tp"),
            P("ep", None, "tp"),
            P("ep", "tp", None),
            P(),
        ),
        out_specs=(P("ep", "tp"), P("ep", None, "tp")),
        check_vma=False,
    )
```
